512 devices in a mesh: sp: 32 (over z, x), tp: 16 (over y, core).
Axes of the slice: x: 4, y: 8, z: 8, core: 2. Of those that a mesh axis runs over, the one named last changes fastest.
Arguments:
- mid_state: bfloat16 [8192, 2048], P('sp'), may hold values from -6 to 6
- conv_pre: bfloat16 [8192, 1024], P('sp', 'tp'), may hold values from -8 to 8
- conv_taps: bfloat16 [31, 1024], P(None, 'tp'), may hold values from -1 to 1
- out_proj: bfloat16 [1024, 2048], P('tp'), may hold values from -0.1875 to 0.1875
- route_expert: int32 [8192, 2], P('sp'), may hold values from 0 to 31, as said below
- route_weight: float32 [8192, 2], P('sp'), may hold values from 0.1 to 1
- gate_w: bfloat16 [32, 2048, 2048], P('sp', None, 'tp'), may hold values from -0.125 to 0.125
- up_w: bfloat16 [32, 2048, 2048], P('sp', None, 'tp'), may hold values from -0.125 to 0.125
- down_w: bfloat16 [32, 2048, 2048], P('sp', 'tp'), may hold values from -0.125 to 0.125
- cotangent: bfloat16 [8192, 2048], P('sp'), may hold values from -6 to 6
Outputs:
- grad_gate: bfloat16 [32, 2048, 2048], P('sp', None, 'tp')
- grad_up: bfloat16 [32, 2048, 2048], P('sp', None, 'tp')
- grad_down: bfloat16 [32, 2048, 2048], P('sp', 'tp')
- grad_proj: float32 [2048, 1024], P('sp', 'tp')
- conv_input_grad: float32 [8192, 1024], P('sp', 'tp')
The draws below stay inside these ranges and needn't reach their ends.
Inputs may be any that keep to these rules, and one draw needn't show every extreme that they name: `route_expert`: the two experts of a token are different and lie in one group of 32 // 4 consecutive experts; in every draw some expert is named by more than 17 routes of every aligned block of 256 tokens.
All inputs are finite; a program needn't handle non-finite values.
Results may differ from the reference program's by a relative error of at most 0.02.
Values may be sent and summed in bfloat16 or wider, within the bound.
A program may use at most 128 MiB of HBM per device.

```python
import jax
import jax.numpy as jnp
from jax import lax

D = 2048
FF = 2048
CONV = 1024
KERNEL = 31
TOP = 2
GROUPS = 4
TOK_DEV = 256
TOKENS = 8192
EXPERTS = 32
SLOTS = 17
N_TP = 16


def draw_route_expert(key, part):
    keys = jax.random.split(jax.random.fold_in(key, 17), 6)
    per_group = EXPERTS // GROUPS
    group_pick = jax.random.randint(keys[0], (TOKENS,), 0, GROUPS)
    first_pick = jax.random.randint(keys[1], (TOKENS,), 0, per_group)
    offset_pick = jax.random.randint(keys[2], (TOKENS,), 0, per_group - 1)
    second_pick = (first_pick + 1 + offset_pick) % per_group
    focus = jax.random.randint(keys[3], (), 0, EXPERTS)
    block_shift = jax.random.randint(keys[4], (TOKENS // TOK_DEV,), 0, TOK_DEV)
    row_ids = jnp.arange(TOKENS, dtype=jnp.int32)
    inside = (row_ids % TOK_DEV - block_shift[row_ids // TOK_DEV]) % TOK_DEV
    forced = inside <= SLOTS
    group_pick = jnp.where(forced, focus // per_group, group_pick)
    first_pick = jnp.where(forced, focus % per_group, first_pick)
    second_pick = jnp.where(forced, (focus % per_group + 1 + offset_pick) % per_group, second_pick)
    return jnp.stack([group_pick * per_group + first_pick, group_pick * per_group + second_pick], axis=1).astype(jnp.int32)


def with_spikes(result, own_key, source, target, blocks, factor):
    owner, partner = [(jnp.arange(result.shape[position]) // (result.shape[position] // blocks)).reshape([-1 if axis == position else 1 for axis in range(result.ndim)]) for position in (source, target)]
    chosen = jax.random.permutation(own_key, blocks)[partner]
    strong = (owner == chosen) | (owner == (partner + blocks // 2) % blocks)
    return jnp.where(strong, factor * result, result)


def levels(stream_key, shape, cuts, smallest, top_value):
    def one(axis_at, shards_of):
        steps = jax.random.uniform(jax.random.fold_in(jax.random.fold_in(stream_key, 6), axis_at), (shards_of,), jnp.float32, smallest / len(cuts), top_value / len(cuts))
        return jnp.repeat(jnp.exp(steps), shape[axis_at] // shards_of).reshape((-1,) + (1,) * (len(shape) - axis_at - 1))

    gain = one(*cuts[0])
    for cut in cuts[1:]:
        gain = gain * one(*cut)
    return gain


def bell_draw(rng, extent, scale, bound, pieces=(), kind=jnp.bfloat16):
    values = jax.random.normal(rng, extent, jnp.float32) * scale
    if len(pieces) > 0:
        values = levels(rng, extent, pieces, -0.22, 0.18) * values
    return jnp.clip(values, min=-bound, max=bound).astype(kind)


def heavy_noise(stream_key, shape, deviation, most, cuts, heavy, held_as=jnp.bfloat16):
    array = deviation * jax.random.normal(stream_key, shape, jnp.float32)
    if cuts:
        array = array * levels(stream_key, shape, cuts, -0.22, 0.18)
    return jnp.clip(with_spikes(array, jax.random.fold_in(stream_key, 3), *heavy), -most, most).astype(held_as)


def setup_inputs(seed: int = 0) -> dict:
    key_list = jax.random.split(jax.random.key(seed), 11)
    mid_state = bell_draw(key_list[0], (TOKENS, D), 1.0, 6.0, ((0, 32),))
    conv_pre = bell_draw(key_list[1], (TOKENS, CONV), 1.5, 8.0, ((0, 32), (1, 16)))
    conv_taps = bell_draw(key_list[2], (KERNEL, CONV), KERNEL ** -0.5, 1.0, ((1, 16),))
    out_proj = bell_draw(key_list[3], (CONV, D), CONV ** -0.5, 0.1875, ((0, 16),))
    route_expert = draw_route_expert(jax.random.fold_in(key_list[10], 71), 0)
    route_weight = jnp.clip(0.1 + 0.9 * jax.random.uniform(key_list[5], (TOKENS, TOP), jnp.float32) ** levels(key_list[5], (TOKENS, TOP), ((0, 32),), -0.2, 0.2), 0.1, 1.0)
    gate_w = bell_draw(key_list[6], (EXPERTS, D, FF), D ** -0.5, 0.125, ((0, 32), (2, 16)))
    up_w = bell_draw(key_list[7], (EXPERTS, D, FF), D ** -0.5, 0.125, ((0, 32), (2, 16)))
    down_w = bell_draw(key_list[8], (EXPERTS, FF, D), FF ** -0.5, 0.125, ((0, 32), (1, 16)))
    cotangent = heavy_noise(key_list[9], (TOKENS, D), 1.0, 6.0, ((0, 32),), (0, 1, 32, 2.75))
    return {"mid_state": mid_state, "conv_pre": conv_pre, "conv_taps": conv_taps, "out_proj": out_proj, "route_expert": route_expert, "route_weight": route_weight, "gate_w": gate_w, "up_w": up_w, "down_w": down_w, "cotangent": cotangent}


def silu_slope(value):
    sig = jax.nn.sigmoid(value)
    return sig * (1.0 + value * (1.0 - sig))


def expert_backward(packed):
    inputs, seeds, gate_mat, up_mat, down_mat = packed
    gate_pre = jnp.dot(inputs, gate_mat, preferred_element_type=jnp.float32)
    up_pre = jnp.dot(inputs, up_mat, preferred_element_type=jnp.float32)
    gate_act = jax.nn.silu(gate_pre)
    hidden = (gate_act * up_pre).astype(jnp.bfloat16)
    grad_down = jnp.dot(hidden.T, seeds, preferred_element_type=jnp.float32).astype(jnp.bfloat16)
    hidden_grad = jnp.dot(seeds, down_mat.T, preferred_element_type=jnp.float32)
    gate_grad = (hidden_grad * up_pre * silu_slope(gate_pre)).astype(jnp.bfloat16)
    up_grad = (hidden_grad * gate_act).astype(jnp.bfloat16)
    grad_gate = jnp.dot(inputs.T, gate_grad, preferred_element_type=jnp.float32).astype(jnp.bfloat16)
    grad_up = jnp.dot(inputs.T, up_grad, preferred_element_type=jnp.float32).astype(jnp.bfloat16)
    slot_total = inputs.shape[0]
    block_width = FF // N_TP
    gate_blocks = gate_grad.astype(jnp.float32).reshape(slot_total, N_TP, block_width)
    up_blocks = up_grad.astype(jnp.float32).reshape(slot_total, N_TP, block_width)
    gate_wblocks = gate_mat.astype(jnp.float32).reshape(D, N_TP, block_width)
    up_wblocks = up_mat.astype(jnp.float32).reshape(D, N_TP, block_width)
    partial_value = jnp.einsum("rjf,djf->rjd", gate_blocks, gate_wblocks) + jnp.einsum("rjf,djf->rjd", up_blocks, up_wblocks)
    partial_value = partial_value.astype(jnp.bfloat16).astype(jnp.float32)
    input_grad = jnp.sum(partial_value, axis=1).astype(jnp.bfloat16)
    return grad_gate, grad_up, grad_down, input_grad


def reference(mid_state, conv_pre, conv_taps, out_proj, route_expert, route_weight, gate_w, up_w, down_w, cotangent):
    blocks = TOKENS // TOK_DEV
    flat_routes = route_expert.reshape(-1)
    one_hot_table = (flat_routes[:, None] == jnp.arange(EXPERTS, dtype=jnp.int32)[None, :]).astype(jnp.int32)
    one_hot_table = one_hot_table.reshape(blocks, TOK_DEV * TOP, EXPERTS)
    slot_rank = (jnp.sum(jnp.cumsum(one_hot_table, axis=1) * one_hot_table, axis=2) - 1).reshape(-1)
    route_ids = jnp.arange(TOKENS * TOP, dtype=jnp.int32)
    source_block = route_ids // (TOK_DEV * TOP)
    token_ids = route_ids // TOP
    kept_mask = slot_rank < SLOTS
    per_expert = blocks * SLOTS
    slot_index = jnp.where(kept_mask, flat_routes * per_expert + source_block * SLOTS + slot_rank, EXPERTS * per_expert).astype(jnp.int32)
    route_cot = (route_weight.reshape(-1)[:, None] * cotangent[token_ids].astype(jnp.float32)).astype(jnp.bfloat16)
    slot_inputs = jnp.zeros((EXPERTS * per_expert, D), jnp.bfloat16).at[slot_index].set(mid_state[token_ids], mode="drop")
    slot_seeds = jnp.zeros((EXPERTS * per_expert, D), jnp.bfloat16).at[slot_index].set(route_cot, mode="drop")
    grad_gate, grad_up, grad_down, input_grad = lax.map(expert_backward, (slot_inputs.reshape(EXPERTS, per_expert, D), slot_seeds.reshape(EXPERTS, per_expert, D), gate_w, up_w, down_w))
    input_flat = input_grad.reshape(EXPERTS * per_expert, D)
    safe_index = jnp.minimum(slot_index, EXPERTS * per_expert - 1)
    returned = jnp.where(kept_mask[:, None], input_flat[safe_index].astype(jnp.float32), jnp.float32(0.0))
    moe_grad = jnp.sum(returned.reshape(TOKENS, TOP, D), axis=1)
    mid_grad = (cotangent.astype(jnp.float32) + moe_grad).astype(jnp.bfloat16)
    pre_float = conv_pre.astype(jnp.float32)
    activated = jax.nn.silu(pre_float).astype(jnp.bfloat16)
    grad_proj = jnp.dot(mid_grad.T, activated, preferred_element_type=jnp.float32)
    mixed_grad = jnp.dot(mid_grad, out_proj.T, preferred_element_type=jnp.float32)
    conv_grad = (mixed_grad * silu_slope(pre_float)).astype(jnp.bfloat16)
    extended = jnp.concatenate([conv_grad.astype(jnp.float32), jnp.zeros((KERNEL - 1, CONV), jnp.float32)], axis=0)
    conv_input_grad = jnp.zeros((TOKENS, CONV), jnp.float32)
    for lag_index in range(KERNEL):
        conv_input_grad = conv_input_grad + conv_taps[lag_index].astype(jnp.float32)[None, :] * extended[lag_index:lag_index + TOKENS]
    return grad_gate, grad_up, grad_down, grad_proj, conv_input_grad
```

```python
import functools

import jax
import jax.numpy as jnp
from jax import lax
from jax.experimental import pallas as pl
from jax.experimental.pallas import tpu as pltpu
from jax.sharding import PartitionSpec as P

KERNEL = 31
LANES = 128
MAIN = 16
MESH = pl.DeviceIdType.MESH
F32 = jnp.float32
BF16 = jnp.bfloat16


def silu_slope(value):
    sig = jax.nn.sigmoid(value)
    return sig * (1.0 + value * (1.0 - sig))


def copy_to(src, dst, send, recv, sp, tp):
    return pltpu.make_async_remote_copy(
        src_ref=src,
        dst_ref=dst,
        send_sem=send,
        recv_sem=recv,
        device_id=(sp, tp),
        device_id_type=MESH,
    )


def moe_kernel(
    S,
    T,
    route_e,
    route_w,
    mid,
    cot,
    gate_w,
    up_w,
    down_w,
    grad_gate,
    grad_up,
    grad_down,
    mid_grad,
    send_main,
    send_ext,
    rows,
    ext,
    ext_flat,
    ext_in,
    ext_seed,
    acc_gu,
    acc_h,
    onehot,
    onehot_x,
    hidden,
    pre_grads,
    sib_out,
    sib_in,
    own_part,
    ring_out,
    ring_in,
    back_main,
    back_ext,
    home_main,
    home_ext,
    gathered,
    a2a_send,
    a2a_recv,
    ag_send,
    ag_recv,
    sib_send,
    sib_recv,
    rsib_send,
    rsib_recv,
    rs_send,
    rs_recv,
    ret_send,
    ret_recv,
    mg_send,
    mg_recv,
    mgs_send,
    mgs_recv,
):
    Y = T // 2
    H = Y // 2
    NQ = ag_recv.shape[2]
    KQ = S // NQ
    R = S * MAIN
    N = R + S
    HALF = N // 2
    TOK = mid.shape[0]
    me = lax.axis_index("sp")
    tp = lax.axis_index("tp")
    y = tp // 2
    core = tp % 2
    sib = tp + 1 - 2 * core
    right = lax.rem(tp + 2, T)
    left = lax.rem(tp + T - 2, T)

    def chunk(i, parity):
        return 2 * lax.rem(y - i + 2 * Y, Y) + parity

    barrier = pltpu.get_barrier_semaphore()

    @pl.loop(1, S)
    def _(k):
        pl.semaphore_signal(
            barrier, inc=1, device_id=(lax.rem(me + k, S), tp), device_id_type=MESH
        )

    for peer in (left, right, sib):
        pl.semaphore_signal(barrier, inc=1, device_id=(me, peer), device_id_type=MESH)

    e_rel = route_e[...] - me
    e_rel = jnp.where(e_rel < 0, e_rel + S, e_rel)
    e_iota = lax.broadcasted_iota(jnp.int32, (S, TOK), 0)
    oh = [e_iota == e_rel[k : k + 1, :] for k in range(2)]
    oh_sum = (oh[0] | oh[1]).astype(F32).astype(BF16)
    before = (
        lax.broadcasted_iota(jnp.int32, (TOK, TOK), 0)
        < lax.broadcasted_iota(jnp.int32, (TOK, TOK), 1)
    ).astype(F32).astype(BF16)
    counts = jnp.dot(oh_sum, before, preferred_element_type=F32)
    main_rows = lax.broadcasted_iota(jnp.int32, (R, TOK), 0)
    ext_rows = lax.broadcasted_iota(jnp.int32, (S, TOK), 0)
    pair_rows = lax.broadcasted_iota(jnp.int32, (2 * S, TOK), 0)
    g_main, g_ext, g_pair = [], [], []
    for k in range(2):
        rank = jnp.sum(jnp.where(oh[k], counts, 0.0), axis=0, keepdims=True).astype(jnp.int32)
        own = e_rel[k : k + 1, :]
        key = jnp.where(rank < MAIN, own * MAIN + rank, -1)
        key_x = jnp.where(rank == MAIN, own, -1)
        g_main.append(main_rows == key)
        g_ext.append(ext_rows == key_x)
        g_pair.append(pair_rows == 2 * key_x + 1)
    w = [route_w[k : k + 1, :] for k in range(2)]
    gm = (g_main[0] | g_main[1]).astype(F32).astype(BF16)
    onehot[...] = gm
    onehot_x[...] = (g_ext[0] | g_ext[1]).astype(F32).astype(BF16)
    col = pl.ds(pl.multiple_of(tp * LANES, LANES), LANES)
    mid_c = mid[:, col]
    cot_c = cot[:, col]
    w_main = jnp.sum(
        jnp.where(g_main[0], w[0], 0.0) + jnp.where(g_main[1], w[1], 0.0), axis=1, keepdims=True
    )
    in_rows = jnp.dot(gm, mid_c, preferred_element_type=F32).astype(BF16)
    seed_rows = (w_main * jnp.dot(gm, cot_c, preferred_element_type=F32)).astype(BF16)
    send_main[:, 0:MAIN, :] = in_rows.reshape(S, MAIN, LANES)
    send_main[:, MAIN : 2 * MAIN, :] = seed_rows.reshape(S, MAIN, LANES)
    w_pair = jnp.sum(
        jnp.where(g_pair[0], w[0], 0.0) + jnp.where(g_pair[1], w[1], 0.0), axis=1, keepdims=True
    )
    g_odd = (g_pair[0] | g_pair[1]).astype(F32).astype(BF16)
    pair_even = lax.broadcasted_iota(jnp.int32, (2 * S, S), 0) == 2 * lax.broadcasted_iota(
        jnp.int32, (2 * S, S), 1
    )
    g_even = jnp.dot(
        pair_even.astype(F32).astype(BF16), onehot_x[...], preferred_element_type=F32
    ).astype(BF16)
    pair_val = (
        jnp.dot(g_even, mid_c, preferred_element_type=F32)
        + w_pair * jnp.dot(g_odd, cot_c, preferred_element_type=F32)
    ).astype(BF16)
    for s in range(S):
        send_ext[s] = pair_val[2 * s : 2 * s + 2, :]

    pl.semaphore_wait(barrier, S + 2)

    @pl.loop(1, S)
    def _(k):
        dst = lax.rem(me + k, S)
        q = k // KQ
        copy_to(
            send_main.at[k], rows.at[tp, k], a2a_send.at[0], a2a_recv.at[0, q], dst, tp
        ).start()
        copy_to(
            send_ext.at[k], ext.at[tp, k], a2a_send.at[1], a2a_recv.at[1, q], dst, tp
        ).start()

    rows[tp, 0] = send_main[0]
    ext[tp, 0] = send_ext[0]

    def sub(ref, j, q):
        return ref.at[j, pl.ds(q * KQ, KQ)]

    both = (rows, ext)

    def ag_copies(d, t, q, j):
        peer = right if d == 0 else left
        return [
            copy_to(
                sub(ref, j, q),
                sub(ref, j, q),
                ag_send.at[d, t, q, b],
                ag_recv.at[d, t, q, b],
                me,
                peer,
            )
            for b, ref in enumerate(both)
        ]

    def sib_copies(i, q, j):
        return [
            copy_to(
                sub(ref, j, q),
                sub(ref, j, q),
                sib_send.at[i, q, b],
                sib_recv.at[i, q, b],
                me,
                sib,
            )
            for b, ref in enumerate(both)
        ]

    def carries(d, t, q):
        if t + 1 < H:
            return True
        if t + 1 > H:
            return False
        return (q < NQ // 2) == (d == 0)

    sent = []

    def start_all(copies):
        for c in copies:
            c.start()
        sent.extend(copies)

    for q in range(NQ):
        lo = 1 if q == 0 else q * KQ
        n = (q + 1) * KQ - lo
        if n > 0:
            for b, (src, ref) in enumerate(((send_main, rows), (send_ext, ext))):
                copy_to(
                    src.at[pl.ds(lo, n)],
                    ref.at[tp, pl.ds(lo, n)],
                    a2a_send.at[b],
                    a2a_recv.at[b, q],
                    me,
                    sib,
                ).wait_recv()
        for d in range(2):
            if carries(d, 0, q):
                start_all(ag_copies(d, 0, q, tp))
        start_all(sib_copies(0, q, tp))

    sel_row = lax.broadcasted_iota(jnp.int32, (S, 2 * S), 0)
    sel_col = lax.broadcasted_iota(jnp.int32, (S, 2 * S), 1)
    sels = [(sel_col == 2 * sel_row + b).astype(F32).astype(BF16) for b in range(2)]
    acc_gu[...] = jnp.zeros_like(acc_gu)
    acc_h[...] = jnp.zeros_like(acc_h)

    def in_value(j):
        return jnp.concatenate(
            [rows[j, :, 0:MAIN, :].reshape(R, LANES), ext_in[j]], axis=0
        )

    def seed_value(j):
        return jnp.concatenate(
            [rows[j, :, MAIN : 2 * MAIN, :].reshape(R, LANES), ext_seed[j]], axis=0
        )

    def use_pair(i):
        for q in range(NQ):
            for c in sib_copies(i, q, chunk(i, 1 - core)):
                c.wait_recv()
        j0 = chunk(i, 0)
        for p in range(2):
            j = j0 + p
            for s in range(S):
                ext_flat[2 * s : 2 * s + 2, :] = ext[j, s]
            flat = ext_flat[...]
            ext_in[j] = jnp.dot(sels[0], flat, preferred_element_type=F32).astype(BF16)
            ext_seed[j] = jnp.dot(sels[1], flat, preferred_element_type=F32).astype(BF16)
        span = pl.ds(pl.multiple_of(j0 * LANES, 2 * LANES), 2 * LANES)
        w_gu = jnp.concatenate([gate_w[span, :], up_w[span, :]], axis=1)
        x = jnp.concatenate([in_value(j0), in_value(j0 + 1)], axis=1)
        acc_gu[...] += jnp.dot(x, w_gu, preferred_element_type=F32)
        g = jnp.concatenate([seed_value(j0), seed_value(j0 + 1)], axis=1)
        acc_h[...] += lax.dot_general(
            g, down_w[:, span], (((1,), (1,)), ((), ())), preferred_element_type=F32
        )

    use_pair(0)
    for t in range(H):
        for q in range(NQ):
            for d in range(2):
                if not carries(d, t, q):
                    continue
                i = t + 1 if d == 0 else Y - (t + 1)
                j = chunk(i, core)
                for c in ag_copies(d, t, q, j):
                    c.wait_recv()
                if carries(d, t + 1, q):
                    start_all(ag_copies(d, t + 1, q, j))
                start_all(sib_copies(i, q, j))
        if t + 1 < H:
            use_pair(t + 1)
            use_pair(Y - (t + 1))
        else:
            use_pair(H)

    gate_pre = acc_gu[:, 0:LANES]
    up_pre = acc_gu[:, LANES : 2 * LANES]
    h_grad = acc_h[...]
    sig = jax.nn.sigmoid(gate_pre)
    act = gate_pre * sig
    hidden[...] = (act * up_pre).astype(BF16)
    pre_grads[:, 0:LANES] = (
        h_grad * up_pre * (sig * (1.0 + gate_pre * (1.0 - sig)))
    ).astype(BF16)
    pre_grads[:, LANES : 2 * LANES] = (h_grad * act).astype(BF16)

    def partial(j):
        span = pl.ds(pl.multiple_of(j * LANES, LANES), LANES)
        w_gu = jnp.concatenate([gate_w[span, :], up_w[span, :]], axis=1)
        return lax.dot_general(
            pre_grads[...], w_gu, (((1,), (1,)), ((), ())), preferred_element_type=F32
        )

    order = [H] + [o for d in range(H - 1, 0, -1) for o in (d, Y - d)] + [0]
    if H == 0:
        order = [0]

    def dest(o, parity):
        return 2 * lax.rem(y + o, Y) + parity

    def rsib_copy(o):
        return copy_to(
            sib_out.at[o], sib_in.at[o], rsib_send.at[o], rsib_recv.at[o], me, sib
        )

    for o in order:
        sib_out[o] = partial(dest(o, 1 - core)).astype(BF16)
        start_all([rsib_copy(o)])

    def weight_grads(j):
        span = pl.ds(pl.multiple_of(j * LANES, LANES), LANES)
        both_g = lax.dot_general(
            in_value(j), pre_grads[...], (((0,), (0,)), ((), ())), preferred_element_type=F32
        ).astype(BF16)
        grad_gate[span, :] = both_g[:, 0:LANES]
        grad_up[span, :] = both_g[:, LANES : 2 * LANES]
        grad_down[:, span] = lax.dot_general(
            hidden[...], seed_value(j), (((0,), (0,)), ((), ())), preferred_element_type=F32
        ).astype(BF16)

    for o in order:
        own_part[o] = partial(dest(o, core))

    def half(h):
        return pl.ds(h * HALF, HALF)

    def rs_copy(d, t, h):
        return copy_to(
            ring_out.at[d, t, h],
            ring_in.at[d, t, h],
            rs_send.at[d, t, h],
            rs_recv.at[d, t, h],
            me,
            right if d == 0 else left,
        )

    def rs_has(d, t, h):
        if t < 0:
            return False
        return t > 0 or h == d

    done = 0
    for t in range(H):
        dist = H - t
        for h in range(2):
            for d in range(2):
                if not rs_has(d, t, h):
                    continue
                o = dist if d == 0 else Y - dist
                if (d == 0 or dist < H) and h == (d if t == 0 else 0):
                    rsib_copy(o).wait_recv()
                value = own_part[o, half(h), :] + sib_in[o, half(h), :].astype(F32)
                if rs_has(d, t - 1, h):
                    rs_copy(d, t - 1, h).wait_recv()
                    value = value + ring_in[d, t - 1, h].astype(F32)
                ring_out[d, t, h] = value.astype(BF16)
                start_all([rs_copy(d, t, h)])
        stop = T * (t + 1) // H

        @pl.loop(done, stop)
        def _(j):
            weight_grads(j)

        done = stop

    rsib_copy(0).wait_recv()
    for h in range(2):
        value = own_part[0, half(h), :] + sib_in[0, half(h), :].astype(F32)
        for d in range(2):
            if rs_has(d, H - 1, h):
                rs_copy(d, H - 1, h).wait_recv()
                value = value + ring_in[d, H - 1, h].astype(F32)
        own_part[0, half(h), :] = value
    back_main[...] = own_part[0, 0:R, :].astype(BF16).reshape(S, MAIN, LANES)
    last = own_part[0, R:N, :].astype(BF16).astype(F32)
    for s in range(S):
        back_ext[s] = last[s : s + 1, :]

    @pl.loop(1, S)
    def _(k):
        dst = lax.rem(me + S - k, S)
        copy_to(
            back_main.at[k], home_main.at[k], ret_send.at[0], ret_recv.at[0], dst, tp
        ).start()
        copy_to(
            back_ext.at[k], home_ext.at[k], ret_send.at[1], ret_recv.at[1], dst, tp
        ).start()

    home_main[0] = back_main[0]
    home_ext[0] = back_ext[0]
    if S > 1:
        for b, (src, ref) in enumerate(((back_main, home_main), (back_ext, home_ext))):
            copy_to(
                src.at[pl.ds(1, S - 1)],
                ref.at[pl.ds(1, S - 1)],
                ret_send.at[b],
                ret_recv.at[b],
                me,
                sib,
            ).wait()
        for b, (src, ref) in enumerate(((send_main, rows), (send_ext, ext))):
            copy_to(
                src.at[pl.ds(1, S - 1)],
                ref.at[tp, pl.ds(1, S - 1)],
                a2a_send.at[b],
                a2a_recv.at[b, 0],
                me,
                sib,
            ).wait_send()
    home_x = jnp.concatenate([home_ext[s] for s in range(S)], axis=0).astype(BF16)
    moe = lax.dot_general(
        onehot[...],
        home_main[...].reshape(R, LANES),
        (((0,), (0,)), ((), ())),
        preferred_element_type=F32,
    ) + lax.dot_general(
        onehot_x[...], home_x, (((0,), (0,)), ((), ())), preferred_element_type=F32
    )
    gathered[tp] = (cot[:, col].astype(F32) + moe).astype(BF16)

    TH = TOK // 2

    def mg_copy(d, t, h, j):
        part = gathered.at[j, pl.ds(h * TH, TH)]
        return copy_to(
            part,
            part,
            mg_send.at[d, t, h],
            mg_recv.at[d, t, h],
            me,
            right if d == 0 else left,
        )

    def mgs_copy(i, h, j):
        part = gathered.at[j, pl.ds(h * TH, TH)]
        return copy_to(part, part, mgs_send.at[i, h], mgs_recv.at[i, h], me, sib)

    def mg_carries(d, t, h):
        if t + 1 < H:
            return True
        if t + 1 > H:
            return False
        return h == d

    for h in range(2):
        for d in range(2):
            if mg_carries(d, 0, h):
                start_all([mg_copy(d, 0, h, tp)])
        start_all([mgs_copy(0, h, tp)])
    for t in range(H):
        for h in range(2):
            for d in range(2):
                if not mg_carries(d, t, h):
                    continue
                i = t + 1 if d == 0 else Y - (t + 1)
                j = chunk(i, core)
                mg_copy(d, t, h, j).wait_recv()
                if mg_carries(d, t + 1, h):
                    start_all([mg_copy(d, t + 1, h, j)])
                start_all([mgs_copy(i, h, j)])
    for i in range(Y):
        for h in range(2):
            mgs_copy(i, h, chunk(i, 1 - core)).wait_recv()
    for j in range(T):
        mid_grad[:, j * LANES : (j + 1) * LANES] = gathered[j]
    for c in sent:
        c.wait_send()


def moe_call(S, T, route_e, route_w, mid, cot, gate_w, up_w, down_w):
    Y = T // 2
    H = Y // 2
    TOK, D = mid.shape
    NQ = min(4, S)
    R = S * MAIN
    N = R + S
    vmem = pl.BlockSpec(memory_space=pltpu.VMEM)
    dma = pltpu.SemaphoreType.DMA
    scratch = [
        pltpu.VMEM((S, 2 * MAIN, LANES), BF16),
        pltpu.VMEM((S, 2, LANES), BF16),
        pltpu.VMEM((T, S, 2 * MAIN, LANES), BF16),
        pltpu.VMEM((T, S, 2, LANES), BF16),
        pltpu.VMEM((2 * S, LANES), BF16),
        pltpu.VMEM((T, S, LANES), BF16),
        pltpu.VMEM((T, S, LANES), BF16),
        pltpu.VMEM((N, 2 * LANES), F32),
        pltpu.VMEM((N, LANES), F32),
        pltpu.VMEM((R, TOK), BF16),
        pltpu.VMEM((S, TOK), BF16),
        pltpu.VMEM((N, LANES), BF16),
        pltpu.VMEM((N, 2 * LANES), BF16),
        pltpu.VMEM((Y, N, LANES), BF16),
        pltpu.VMEM((Y, N, LANES), BF16),
        pltpu.VMEM((Y, N, LANES), F32),
        pltpu.VMEM((2, H, 2, N // 2, LANES), BF16),
        pltpu.VMEM((2, H, 2, N // 2, LANES), BF16),
        pltpu.VMEM((S, MAIN, LANES), BF16),
        pltpu.VMEM((S, 1, LANES), F32),
        pltpu.VMEM((S, MAIN, LANES), BF16),
        pltpu.VMEM((S, 1, LANES), F32),
        pltpu.VMEM((T, TOK, LANES), BF16),
        dma((2,)),
        dma((2, NQ)),
        dma((2, H, NQ, 2)),
        dma((2, H, NQ, 2)),
        dma((Y, NQ, 2)),
        dma((Y, NQ, 2)),
        dma((Y,)),
        dma((Y,)),
        dma((2, H, 2)),
        dma((2, H, 2)),
        dma((2,)),
        dma((2,)),
        dma((2, H, 2)),
        dma((2, H, 2)),
        dma((Y, 2)),
        dma((Y, 2)),
    ]
    return pl.pallas_call(
        functools.partial(moe_kernel, S, T),
        out_shape=(
            jax.ShapeDtypeStruct((D, LANES), BF16),
            jax.ShapeDtypeStruct((D, LANES), BF16),
            jax.ShapeDtypeStruct((LANES, D), BF16),
            jax.ShapeDtypeStruct((TOK, D), BF16),
        ),
        in_specs=[vmem] * 7,
        out_specs=(vmem,) * 4,
        scratch_shapes=scratch,
        compiler_params=pltpu.CompilerParams(
            collective_id=0, has_side_effects=True, vmem_limit_bytes=60 * 1024 * 1024
        ),
    )(route_e, route_w, mid, cot, gate_w, up_w, down_w)


def split_up(shard, dim, peers):
    shape = shard.shape
    parts = shard.reshape(*shape[:dim], peers, shape[dim] // peers, *shape[dim + 1 :])
    return jnp.moveaxis(parts, dim, 0)


def sum_at_owner(shard, axis, dim):
    peers = lax.axis_size(axis)
    parts = lax.all_to_all(split_up(shard, dim, peers), axis, 0, 0, tiled=True)
    return jnp.sum(parts.astype(jnp.float32), axis=0)


def passed_along(value, axis, steps):
    count = lax.axis_size(axis)
    initial, last = (max(0, -steps), min(count, count - steps))
    return lax.ppermute(value, axis, [(source, source + steps) for source in range(initial, last)])


def body(
    S,
    T,
    mid_state,
    conv_pre,
    conv_taps,
    out_proj,
    route_expert,
    route_weight,
    gate_w,
    up_w,
    down_w,
    cotangent,
):
    token_count = mid_state.shape[0]
    grad_gate, grad_up, grad_down, mid_grad = moe_call(
        S,
        T,
        route_expert.T,
        route_weight.T,
        mid_state,
        cotangent,
        gate_w[0],
        up_w[0],
        down_w[0],
    )
    pre_float = conv_pre.astype(jnp.float32)
    activated = jax.nn.silu(pre_float).astype(jnp.bfloat16)
    mixed_grad = lax.dot_general(
        mid_grad, out_proj, (((1,), (1,)), ((), ())), preferred_element_type=jnp.float32
    )
    conv_grad = (mixed_grad * silu_slope(pre_float)).astype(jnp.bfloat16)
    next_head = passed_along(conv_grad[: KERNEL - 1], "sp", -1)
    extended = jnp.concatenate([conv_grad, next_head], axis=0).astype(jnp.float32)
    conv_input_grad = jnp.zeros(conv_grad.shape, jnp.float32)
    for lag_index in range(KERNEL):
        conv_input_grad = (
            conv_input_grad
            + conv_taps[lag_index].astype(jnp.float32)[None, :]
            * extended[lag_index : lag_index + token_count]
        )
    grad_proj = sum_at_owner(
        lax.dot_general(
            mid_grad, activated, (((0,), (0,)), ((), ())), preferred_element_type=jnp.float32
        ).astype(jnp.bfloat16),
        "sp",
        0,
    )
    return (grad_gate[None], grad_up[None], grad_down[None], grad_proj, conv_input_grad)


def solution(mesh):
    placed = (
        P("sp", None),
        P("sp", "tp"),
        P(None, "tp"),
        P("tp", None),
        P("sp", None),
        P("sp", None),
        P("sp", None, "tp"),
        P("sp", None, "tp"),
        P("sp", "tp", None),
        P("sp", None),
    )
    return jax.shard_map(
        functools.partial(body, mesh.shape["sp"], mesh.shape["tp"]),
        mesh=mesh,
        in_specs=placed,
        out_specs=(
            P("sp", None, "tp"),
            P("sp", None, "tp"),
            P("sp", "tp", None),
            P("sp", "tp"),
            P("sp", "tp"),
        ),
        check_vma=False,
    )
```

```python
import functools

import jax
import jax.numpy as jnp
from jax import lax
from jax.experimental import pallas as pl
from jax.experimental.pallas import tpu as pltpu
from jax.sharding import PartitionSpec as P

KERNEL = 31
LANES = 128
MAIN = 16
MESH = pl.DeviceIdType.MESH
F32 = jnp.float32
BF16 = jnp.bfloat16


def copy_to(src, dst, send, recv, sp, tp):
    return pltpu.make_async_remote_copy(
        src_ref=src,
        dst_ref=dst,
        send_sem=send,
        recv_sem=recv,
        device_id=(sp, tp),
        device_id_type=MESH,
    )


def moe_kernel(
    S,
    T,
    route_e,
    route_w,
    mid,
    cot,
    gate_w,
    up_w,
    down_w,
    conv_pre,
    conv_taps,
    out_proj,
    grad_gate,
    grad_up,
    grad_down,
    grad_proj,
    conv_in_grad,
    send_main,
    send_ext,
    rows,
    ext,
    ext_flat,
    ext_in,
    ext_seed,
    acc_gu,
    acc_h,
    onehot,
    onehot_x,
    hidden,
    pre_grads,
    sib_out,
    sib_in,
    own_part,
    ring_out,
    ring_in,
    back_main,
    back_ext,
    home_main,
    home_ext,
    gathered,
    mixed,
    proj_out,
    proj_in,
    halo_out,
    halo_in,
    a2a_send,
    a2a_recv,
    ag_send,
    ag_recv,
    sib_send,
    sib_recv,
    rsib_send,
    rsib_recv,
    rs_send,
    rs_recv,
    ret_send,
    ret_recv,
    mg_send,
    mg_recv,
    mgs_send,
    mgs_recv,
    proj_send,
    proj_recv,
    halo_send,
    halo_recv,
):
    Y = T // 2
    H = Y // 2
    NQ = ag_recv.shape[2]
    KQ = S // NQ
    R = S * MAIN
    N = R + S
    HALF = N // 2
    TOK = mid.shape[0]
    CC = conv_pre.shape[0]
    HW = halo_out.shape[1]
    me = lax.axis_index("sp")
    tp = lax.axis_index("tp")
    y = tp // 2
    core = tp % 2
    sib = tp + 1 - 2 * core
    right = lax.rem(tp + 2, T)
    left = lax.rem(tp + T - 2, T)

    def chunk(i, parity):
        return 2 * lax.rem(y - i + 2 * Y, Y) + parity

    barrier = pltpu.get_barrier_semaphore()

    @pl.loop(1, S)
    def _(k):
        pl.semaphore_signal(
            barrier, inc=1, device_id=(lax.rem(me + k, S), tp), device_id_type=MESH
        )

    for peer in (left, right, sib):
        pl.semaphore_signal(barrier, inc=1, device_id=(me, peer), device_id_type=MESH)

    e_rel = route_e[...] - me
    e_rel = jnp.where(e_rel < 0, e_rel + S, e_rel)
    e_iota = lax.broadcasted_iota(jnp.int32, (S, TOK), 0)
    oh = [e_iota == e_rel[k : k + 1, :] for k in range(2)]
    oh_sum = (oh[0] | oh[1]).astype(F32).astype(BF16)
    before = (
        lax.broadcasted_iota(jnp.int32, (TOK, TOK), 0)
        < lax.broadcasted_iota(jnp.int32, (TOK, TOK), 1)
    ).astype(F32).astype(BF16)
    counts = jnp.dot(oh_sum, before, preferred_element_type=F32)
    main_rows = lax.broadcasted_iota(jnp.int32, (R, TOK), 0)
    ext_rows = lax.broadcasted_iota(jnp.int32, (S, TOK), 0)
    pair_rows = lax.broadcasted_iota(jnp.int32, (2 * S, TOK), 0)
    g_main, g_ext, g_pair = [], [], []
    for k in range(2):
        rank = jnp.sum(jnp.where(oh[k], counts, 0.0), axis=0, keepdims=True).astype(jnp.int32)
        own = e_rel[k : k + 1, :]
        key = jnp.where(rank < MAIN, own * MAIN + rank, -1)
        key_x = jnp.where(rank == MAIN, own, -1)
        g_main.append(main_rows == key)
        g_ext.append(ext_rows == key_x)
        g_pair.append(pair_rows == 2 * key_x + 1)
    w = [route_w[k : k + 1, :] for k in range(2)]
    gm = (g_main[0] | g_main[1]).astype(F32).astype(BF16)
    onehot[...] = gm
    onehot_x[...] = (g_ext[0] | g_ext[1]).astype(F32).astype(BF16)
    col = pl.ds(pl.multiple_of(tp * LANES, LANES), LANES)
    mid_c = mid[:, col]
    cot_c = cot[:, col]
    w_main = jnp.sum(
        jnp.where(g_main[0], w[0], 0.0) + jnp.where(g_main[1], w[1], 0.0), axis=1, keepdims=True
    )
    in_rows = jnp.dot(gm, mid_c, preferred_element_type=F32).astype(BF16)
    seed_rows = (w_main * jnp.dot(gm, cot_c, preferred_element_type=F32)).astype(BF16)
    send_main[:, 0:MAIN, :] = in_rows.reshape(S, MAIN, LANES)
    send_main[:, MAIN : 2 * MAIN, :] = seed_rows.reshape(S, MAIN, LANES)
    w_pair = jnp.sum(
        jnp.where(g_pair[0], w[0], 0.0) + jnp.where(g_pair[1], w[1], 0.0), axis=1, keepdims=True
    )
    g_odd = (g_pair[0] | g_pair[1]).astype(F32).astype(BF16)
    pair_even = lax.broadcasted_iota(jnp.int32, (2 * S, S), 0) == 2 * lax.broadcasted_iota(
        jnp.int32, (2 * S, S), 1
    )
    g_even = jnp.dot(
        pair_even.astype(F32).astype(BF16), onehot_x[...], preferred_element_type=F32
    ).astype(BF16)
    pair_val = (
        jnp.dot(g_even, mid_c, preferred_element_type=F32)
        + w_pair * jnp.dot(g_odd, cot_c, preferred_element_type=F32)
    ).astype(BF16)
    for s in range(S):
        send_ext[s] = pair_val[2 * s : 2 * s + 2, :]

    pl.semaphore_wait(barrier, S + 2)

    @pl.loop(1, S)
    def _(k):
        dst = lax.rem(me + k, S)
        q = k // KQ
        copy_to(
            send_main.at[k], rows.at[tp, k], a2a_send.at[0], a2a_recv.at[0, q], dst, tp
        ).start()
        copy_to(
            send_ext.at[k], ext.at[tp, k], a2a_send.at[1], a2a_recv.at[1, q], dst, tp
        ).start()

    rows[tp, 0] = send_main[0]
    ext[tp, 0] = send_ext[0]

    def sub(ref, j, q):
        return ref.at[j, pl.ds(q * KQ, KQ)]

    both = (rows, ext)

    def ag_copies(d, t, q, j):
        peer = right if d == 0 else left
        return [
            copy_to(
                sub(ref, j, q),
                sub(ref, j, q),
                ag_send.at[d, t, q, b],
                ag_recv.at[d, t, q, b],
                me,
                peer,
            )
            for b, ref in enumerate(both)
        ]

    def sib_copies(i, q, j):
        return [
            copy_to(
                sub(ref, j, q),
                sub(ref, j, q),
                sib_send.at[i, q, b],
                sib_recv.at[i, q, b],
                me,
                sib,
            )
            for b, ref in enumerate(both)
        ]

    def carries(d, t, q):
        if t + 1 < H:
            return True
        if t + 1 > H:
            return False
        return (q < NQ // 2) == (d == 0)

    sent = []

    def start_all(copies):
        for c in copies:
            c.start()
        sent.extend(copies)

    for q in range(NQ):
        lo = 1 if q == 0 else q * KQ
        n = (q + 1) * KQ - lo
        if n > 0:
            for b, (src, ref) in enumerate(((send_main, rows), (send_ext, ext))):
                copy_to(
                    src.at[pl.ds(lo, n)],
                    ref.at[tp, pl.ds(lo, n)],
                    a2a_send.at[b],
                    a2a_recv.at[b, q],
                    me,
                    sib,
                ).wait_recv()
        for d in range(2):
            if carries(d, 0, q):
                start_all(ag_copies(d, 0, q, tp))
        start_all(sib_copies(0, q, tp))

    sel_row = lax.broadcasted_iota(jnp.int32, (S, 2 * S), 0)
    sel_col = lax.broadcasted_iota(jnp.int32, (S, 2 * S), 1)
    sels = [(sel_col == 2 * sel_row + b).astype(F32).astype(BF16) for b in range(2)]
    acc_gu[...] = jnp.zeros_like(acc_gu)
    acc_h[...] = jnp.zeros_like(acc_h)

    def in_value(j):
        return jnp.concatenate(
            [rows[j, :, 0:MAIN, :].reshape(R, LANES), ext_in[j]], axis=0
        )

    def seed_value(j):
        return jnp.concatenate(
            [rows[j, :, MAIN : 2 * MAIN, :].reshape(R, LANES), ext_seed[j]], axis=0
        )

    def use_pair(i):
        for q in range(NQ):
            for c in sib_copies(i, q, chunk(i, 1 - core)):
                c.wait_recv()
        j0 = chunk(i, 0)
        for p in range(2):
            j = j0 + p
            for s in range(S):
                ext_flat[2 * s : 2 * s + 2, :] = ext[j, s]
            flat = ext_flat[...]
            ext_in[j] = jnp.dot(sels[0], flat, preferred_element_type=F32).astype(BF16)
            ext_seed[j] = jnp.dot(sels[1], flat, preferred_element_type=F32).astype(BF16)
        span = pl.ds(pl.multiple_of(j0 * LANES, 2 * LANES), 2 * LANES)
        w_gu = jnp.concatenate([gate_w[span, :], up_w[span, :]], axis=1)
        x = jnp.concatenate([in_value(j0), in_value(j0 + 1)], axis=1)
        acc_gu[...] += jnp.dot(x, w_gu, preferred_element_type=F32)
        g = jnp.concatenate([seed_value(j0), seed_value(j0 + 1)], axis=1)
        acc_h[...] += lax.dot_general(
            g, down_w[:, span], (((1,), (1,)), ((), ())), preferred_element_type=F32
        )

    use_pair(0)
    for t in range(H):
        for q in range(NQ):
            for d in range(2):
                if not carries(d, t, q):
                    continue
                i = t + 1 if d == 0 else Y - (t + 1)
                j = chunk(i, core)
                for c in ag_copies(d, t, q, j):
                    c.wait_recv()
                if carries(d, t + 1, q):
                    start_all(ag_copies(d, t + 1, q, j))
                start_all(sib_copies(i, q, j))
        if t + 1 < H:
            use_pair(t + 1)
            use_pair(Y - (t + 1))
        else:
            use_pair(H)

    gate_pre = acc_gu[:, 0:LANES]
    up_pre = acc_gu[:, LANES : 2 * LANES]
    h_grad = acc_h[...]
    sig = jax.nn.sigmoid(gate_pre)
    act = gate_pre * sig
    hidden[...] = (act * up_pre).astype(BF16)
    pre_grads[:, 0:LANES] = (
        h_grad * up_pre * (sig * (1.0 + gate_pre * (1.0 - sig)))
    ).astype(BF16)
    pre_grads[:, LANES : 2 * LANES] = (h_grad * act).astype(BF16)

    def partial(j):
        span = pl.ds(pl.multiple_of(j * LANES, LANES), LANES)
        w_gu = jnp.concatenate([gate_w[span, :], up_w[span, :]], axis=1)
        return lax.dot_general(
            pre_grads[...], w_gu, (((1,), (1,)), ((), ())), preferred_element_type=F32
        )

    order = [H] + [o for d in range(H - 1, 0, -1) for o in (d, Y - d)] + [0]
    if H == 0:
        order = [0]

    def dest(o, parity):
        return 2 * lax.rem(y + o, Y) + parity

    def rsib_copy(o):
        return copy_to(
            sib_out.at[o], sib_in.at[o], rsib_send.at[o], rsib_recv.at[o], me, sib
        )

    for o in order:
        sib_out[o] = partial(dest(o, 1 - core)).astype(BF16)
        start_all([rsib_copy(o)])

    def weight_grads(j):
        span = pl.ds(pl.multiple_of(j * LANES, LANES), LANES)
        both_g = lax.dot_general(
            in_value(j), pre_grads[...], (((0,), (0,)), ((), ())), preferred_element_type=F32
        ).astype(BF16)
        grad_gate[span, :] = both_g[:, 0:LANES]
        grad_up[span, :] = both_g[:, LANES : 2 * LANES]
        grad_down[:, span] = lax.dot_general(
            hidden[...], seed_value(j), (((0,), (0,)), ((), ())), preferred_element_type=F32
        ).astype(BF16)

    for o in order:
        own_part[o] = partial(dest(o, core))

    def half(h):
        return pl.ds(h * HALF, HALF)

    def rs_copy(d, t, h):
        return copy_to(
            ring_out.at[d, t, h],
            ring_in.at[d, t, h],
            rs_send.at[d, t, h],
            rs_recv.at[d, t, h],
            me,
            right if d == 0 else left,
        )

    def rs_has(d, t, h):
        if t < 0:
            return False
        return t > 0 or h == d

    done = 0
    for t in range(H):
        dist = H - t
        for h in range(2):
            for d in range(2):
                if not rs_has(d, t, h):
                    continue
                o = dist if d == 0 else Y - dist
                if (d == 0 or dist < H) and h == (d if t == 0 else 0):
                    rsib_copy(o).wait_recv()
                value = own_part[o, half(h), :] + sib_in[o, half(h), :].astype(F32)
                if rs_has(d, t - 1, h):
                    rs_copy(d, t - 1, h).wait_recv()
                    value = value + ring_in[d, t - 1, h].astype(F32)
                ring_out[d, t, h] = value.astype(BF16)
                start_all([rs_copy(d, t, h)])
        stop = T * (t + 1) // H

        @pl.loop(done, stop)
        def _(j):
            weight_grads(j)

        done = stop

    rsib_copy(0).wait_recv()
    for h in range(2):
        value = own_part[0, half(h), :] + sib_in[0, half(h), :].astype(F32)
        for d in range(2):
            if rs_has(d, H - 1, h):
                rs_copy(d, H - 1, h).wait_recv()
                value = value + ring_in[d, H - 1, h].astype(F32)
        own_part[0, half(h), :] = value
    back_main[...] = own_part[0, 0:R, :].astype(BF16).reshape(S, MAIN, LANES)
    last = own_part[0, R:N, :].astype(BF16).astype(F32)
    for s in range(S):
        back_ext[s] = last[s : s + 1, :]

    @pl.loop(1, S)
    def _(k):
        dst = lax.rem(me + S - k, S)
        copy_to(
            back_main.at[k], home_main.at[k], ret_send.at[0], ret_recv.at[0], dst, tp
        ).start()
        copy_to(
            back_ext.at[k], home_ext.at[k], ret_send.at[1], ret_recv.at[1], dst, tp
        ).start()

    home_main[0] = back_main[0]
    home_ext[0] = back_ext[0]
    if S > 1:
        for b, (src, ref) in enumerate(((back_main, home_main), (back_ext, home_ext))):
            copy_to(
                src.at[pl.ds(1, S - 1)],
                ref.at[pl.ds(1, S - 1)],
                ret_send.at[b],
                ret_recv.at[b],
                me,
                sib,
            ).wait()
        for b, (src, ref) in enumerate(((send_main, rows), (send_ext, ext))):
            copy_to(
                src.at[pl.ds(1, S - 1)],
                ref.at[tp, pl.ds(1, S - 1)],
                a2a_send.at[b],
                a2a_recv.at[b, 0],
                me,
                sib,
            ).wait_send()
    home_x = jnp.concatenate([home_ext[s] for s in range(S)], axis=0).astype(BF16)
    moe = lax.dot_general(
        onehot[...],
        home_main[...].reshape(R, LANES),
        (((0,), (0,)), ((), ())),
        preferred_element_type=F32,
    ) + lax.dot_general(
        onehot_x[...], home_x, (((0,), (0,)), ((), ())), preferred_element_type=F32
    )
    gathered[tp] = (cot[:, col].astype(F32) + moe).astype(BF16)

    TH = TOK // 2

    def mg_copy(d, t, h, j):
        part = gathered.at[j, pl.ds(h * TH, TH)]
        return copy_to(
            part,
            part,
            mg_send.at[d, t, h],
            mg_recv.at[d, t, h],
            me,
            right if d == 0 else left,
        )

    def mgs_copy(i, h, j):
        part = gathered.at[j, pl.ds(h * TH, TH)]
        return copy_to(part, part, mgs_send.at[i, h], mgs_recv.at[i, h], me, sib)

    def mg_carries(d, t, h):
        if t + 1 < H:
            return True
        if t + 1 > H:
            return False
        return h == d

    pre = conv_pre[...].astype(F32)
    pre_sig = jax.nn.sigmoid(pre)
    activated = (pre * pre_sig).astype(BF16)
    mixed[...] = jnp.zeros_like(mixed)
    units = proj_out.shape[0] // S
    low = lax.broadcasted_iota(jnp.int32, (CC // 2, LANES), 1) < LANES // 2

    def use_mid(i):
        for h in range(2):
            mgs_copy(i, h, chunk(i, 1 - core)).wait_recv()
        j0 = chunk(i, 0)
        span = pl.ds(pl.multiple_of(j0 * LANES, 2 * LANES), 2 * LANES)
        g = jnp.concatenate([gathered[j0], gathered[j0 + 1]], axis=1)
        mixed[...] += lax.dot_general(
            out_proj[:, span], g, (((1,), (1,)), ((), ())), preferred_element_type=F32
        )
        part = jnp.dot(activated, g, preferred_element_type=F32)
        for p in range(2):
            top = part[0 : CC // 2, p * LANES : (p + 1) * LANES]
            low_c = part[CC // 2 : CC, p * LANES : (p + 1) * LANES]
            proj_out[2 * (j0 + p)] = jnp.where(
                low, top, pltpu.roll(low_c, LANES // 2, 1)
            ).astype(BF16)
            proj_out[2 * (j0 + p) + 1] = jnp.where(
                low, pltpu.roll(top, LANES // 2, 1), low_c
            ).astype(BF16)

    for h in range(2):
        for d in range(2):
            if mg_carries(d, 0, h):
                start_all([mg_copy(d, 0, h, tp)])
        start_all([mgs_copy(0, h, tp)])
    use_mid(0)
    for t in range(H):
        for h in range(2):
            for d in range(2):
                if not mg_carries(d, t, h):
                    continue
                i = t + 1 if d == 0 else Y - (t + 1)
                j = chunk(i, core)
                mg_copy(d, t, h, j).wait_recv()
                if mg_carries(d, t + 1, h):
                    start_all([mg_copy(d, t + 1, h, j)])
                start_all([mgs_copy(i, h, j)])
        if t + 1 < H:
            use_mid(t + 1)
            use_mid(Y - (t + 1))
        else:
            use_mid(H)

    conv_grad = (mixed[...] * (pre_sig * (1.0 + pre * (1.0 - pre_sig)))).astype(BF16)
    halo_out[...] = conv_grad[:, 0:HW]
    halo = copy_to(
        halo_out, halo_in, halo_send.at[0], halo_recv.at[0], lax.rem(me + S - 1, S), tp
    )
    if S > 1:
        start_all([halo])

    def block(ref, n):
        return ref.at[pl.ds(n * units, units)]

    @pl.loop(1, S)
    def _(k):
        dst = lax.rem(me + k, S)
        copy_to(
            block(proj_out, dst), block(proj_in, k), proj_send.at[0], proj_recv.at[0], dst, tp
        ).start()

    eye = (
        lax.broadcasted_iota(jnp.int32, (KERNEL, KERNEL), 0)
        == lax.broadcasted_iota(jnp.int32, (KERNEL, KERNEL), 1)
    ).astype(F32).astype(BF16)
    taps = lax.dot_general(
        conv_taps[...], eye, (((0,), (0,)), ((), ())), preferred_element_type=F32
    )
    halo.wait_recv()
    beyond = jnp.where(me == S - 1, 0.0, halo_in[...].astype(F32))
    extended = jnp.concatenate([conv_grad.astype(F32), beyond], axis=1)
    total = taps[:, 0:1] * extended[:, 0:TOK]
    for lag in range(1, KERNEL):
        shifted = pltpu.roll(extended, TOK + HW - lag, 1)
        total = total + taps[:, lag : lag + 1] * shifted[:, 0:TOK]
    conv_in_grad[...] = total

    if S > 1:
        copy_to(
            proj_out.at[pl.ds(units, (S - 1) * units)],
            proj_in.at[pl.ds(units, (S - 1) * units)],
            proj_send.at[0],
            proj_recv.at[0],
            me,
            sib,
        ).wait()
    for u in range(units):
        z = proj_out[me * units + u].astype(F32)
        for k in range(1, S):
            z = z + proj_in[k * units + u].astype(F32)
        tall = jnp.concatenate([z, pltpu.roll(z, LANES // 2, 1)], axis=0)
        grad_proj[u * (LANES // 2) : (u + 1) * (LANES // 2), :] = tall.T[0 : LANES // 2, :]
    for c in sent:
        c.wait_send()


def moe_call(S, T, *args):
    Y = T // 2
    H = Y // 2
    TOK, D = args[2].shape
    CC = args[7].shape[0]
    NQ = min(4, S)
    R = S * MAIN
    N = R + S
    vmem = pl.BlockSpec(memory_space=pltpu.VMEM)
    dma = pltpu.SemaphoreType.DMA
    scratch = [
        pltpu.VMEM((S, 2 * MAIN, LANES), BF16),
        pltpu.VMEM((S, 2, LANES), BF16),
        pltpu.VMEM((T, S, 2 * MAIN, LANES), BF16),
        pltpu.VMEM((T, S, 2, LANES), BF16),
        pltpu.VMEM((2 * S, LANES), BF16),
        pltpu.VMEM((T, S, LANES), BF16),
        pltpu.VMEM((T, S, LANES), BF16),
        pltpu.VMEM((N, 2 * LANES), F32),
        pltpu.VMEM((N, LANES), F32),
        pltpu.VMEM((R, TOK), BF16),
        pltpu.VMEM((S, TOK), BF16),
        pltpu.VMEM((N, LANES), BF16),
        pltpu.VMEM((N, 2 * LANES), BF16),
        pltpu.VMEM((Y, N, LANES), BF16),
        pltpu.VMEM((Y, N, LANES), BF16),
        pltpu.VMEM((Y, N, LANES), F32),
        pltpu.VMEM((2, H, 2, N // 2, LANES), BF16),
        pltpu.VMEM((2, H, 2, N // 2, LANES), BF16),
        pltpu.VMEM((S, MAIN, LANES), BF16),
        pltpu.VMEM((S, 1, LANES), F32),
        pltpu.VMEM((S, MAIN, LANES), BF16),
        pltpu.VMEM((S, 1, LANES), F32),
        pltpu.VMEM((T, TOK, LANES), BF16),
        pltpu.VMEM((CC, TOK), F32),
        pltpu.VMEM((2 * T, CC // 2, LANES), BF16),
        pltpu.VMEM((2 * T, CC // 2, LANES), BF16),
        pltpu.VMEM((CC, min(LANES, TOK)), BF16),
        pltpu.VMEM((CC, min(LANES, TOK)), BF16),
        dma((2,)),
        dma((2, NQ)),
        dma((2, H, NQ, 2)),
        dma((2, H, NQ, 2)),
        dma((Y, NQ, 2)),
        dma((Y, NQ, 2)),
        dma((Y,)),
        dma((Y,)),
        dma((2, H, 2)),
        dma((2, H, 2)),
        dma((2,)),
        dma((2,)),
        dma((2, H, 2)),
        dma((2, H, 2)),
        dma((Y, 2)),
        dma((Y, 2)),
        dma((1,)),
        dma((1,)),
        dma((1,)),
        dma((1,)),
    ]
    return pl.pallas_call(
        functools.partial(moe_kernel, S, T),
        out_shape=(
            jax.ShapeDtypeStruct((D, LANES), BF16),
            jax.ShapeDtypeStruct((D, LANES), BF16),
            jax.ShapeDtypeStruct((LANES, D), BF16),
            jax.ShapeDtypeStruct((D // S, CC), F32),
            jax.ShapeDtypeStruct((CC, TOK), F32),
        ),
        in_specs=[vmem] * len(args),
        out_specs=(vmem,) * 5,
        scratch_shapes=scratch,
        compiler_params=pltpu.CompilerParams(
            collective_id=0, has_side_effects=True, vmem_limit_bytes=60 * 1024 * 1024
        ),
    )(*args)


def body(
    S,
    T,
    mid_state,
    conv_pre,
    conv_taps,
    out_proj,
    route_expert,
    route_weight,
    gate_w,
    up_w,
    down_w,
    cotangent,
):
    grad_gate, grad_up, grad_down, grad_proj, conv_in_grad = moe_call(
        S,
        T,
        route_expert.T,
        route_weight.T,
        mid_state,
        cotangent,
        gate_w[0],
        up_w[0],
        down_w[0],
        conv_pre.T,
        conv_taps,
        out_proj,
    )
    return (grad_gate[None], grad_up[None], grad_down[None], grad_proj, conv_in_grad.T)


def solution(mesh):
    placed = (
        P("sp", None),
        P("sp", "tp"),
        P(None, "tp"),
        P("tp", None),
        P("sp", None),
        P("sp", None),
        P("sp", None, "tp"),
        P("sp", None, "tp"),
        P("sp", "tp", None),
        P("sp", None),
    )
    return jax.shard_map(
        functools.partial(body, mesh.shape["sp"], mesh.shape["tp"]),
        mesh=mesh,
        in_specs=placed,
        out_specs=(
            P("sp", None, "tp"),
            P("sp", None, "tp"),
            P("sp", "tp", None),
            P("sp", "tp"),
            P("sp", "tp"),
        ),
        check_vma=False,
    )
```

```python
import functools

import jax
import jax.numpy as jnp
from jax import lax
from jax.experimental import pallas as pl
from jax.experimental.pallas import tpu as pltpu
from jax.sharding import PartitionSpec as P

KERNEL = 31
LANES = 128
MAIN = 16
MESH = pl.DeviceIdType.MESH
F32 = jnp.float32
BF16 = jnp.bfloat16


def copy_to(src, dst, send, recv, sp, tp):
    return pltpu.make_async_remote_copy(
        src_ref=src,
        dst_ref=dst,
        send_sem=send,
        recv_sem=recv,
        device_id=(sp, tp),
        device_id_type=MESH,
    )


def moe_kernel(
    S,
    T,
    NQ,
    route_e_hbm,
    route_w_hbm,
    mid_hbm,
    cot_hbm,
    gate_hbm,
    up_hbm,
    down_hbm,
    conv_pre_hbm,
    conv_taps_hbm,
    out_proj_hbm,
    grad_gate,
    grad_up,
    grad_down,
    grad_proj,
    conv_in_grad,
    route_e,
    route_w,
    mid,
    cot,
    gate_w,
    up_w,
    down_w,
    conv_pre,
    conv_taps,
    out_proj,
    load_sem,
    send_main,
    send_ext,
    rows,
    ext,
    ext_flat,
    ext_in,
    ext_seed,
    onehot,
    onehot_x,
    hid_main,
    hid_ext,
    pre_main,
    pre_ext,
    sib_out,
    sib_in,
    own_part,
    ring_out,
    ring_in,
    back_main,
    back_ext,
    home_main,
    home_ext,
    gathered,
    mixed,
    proj_out,
    proj_in,
    halo_out,
    halo_in,
    a2a_send,
    a2a_recv,
    ag_send,
    ag_recv,
    sib_send,
    sib_recv,
    rsib_send,
    rsib_recv,
    rs_send,
    rs_recv,
    ret_send,
    ret_recv,
    mg_send,
    mg_recv,
    mgs_send,
    mgs_recv,
    proj_send,
    proj_recv,
    halo_send,
    halo_recv,
):
    Y = T // 2
    H = Y // 2
    G = Y // 4
    KQ = S // NQ
    R = S * MAIN
    RQ = KQ * MAIN
    NG = RQ + KQ
    TOK = mid.shape[1]
    CC = conv_pre.shape[0]
    HW = halo_out.shape[1]
    me = lax.axis_index("sp")
    tp = lax.axis_index("tp")
    y = tp // 2
    core = tp % 2
    sib = tp + 1 - 2 * core
    right = lax.rem(tp + 2, T)
    left = lax.rem(tp + T - 2, T)
    peers = (right, left)
    tp2 = lax.rem(tp + H * 2, T)
    mine = (tp, tp2)

    X = 4 if S >= 16 else 1
    Z = S // X
    mz = me // X
    mx = me % X

    def apart(b, sign):
        c = b // X
        zo = jnp.where(c % 2 == 1, (c + 1) // 2, -(c // 2))
        return lax.rem(mz + sign * zo + Z, Z) * X + lax.rem(mx + sign * (b % X) + X, X)

    def chunk(i, parity):
        return 2 * lax.rem(y - i + 2 * Y, Y) + parity

    def lanes(j, width=1):
        return pl.ds(pl.multiple_of(j * LANES, LANES * width), LANES * width)

    barrier = pltpu.get_barrier_semaphore()

    @pl.loop(1, S)
    def _(k):
        pl.semaphore_signal(
            barrier, inc=1, device_id=(apart(k, 1), tp), device_id_type=MESH
        )

    for peer in (left, right, sib):
        pl.semaphore_signal(barrier, inc=1, device_id=(me, peer), device_id_type=MESH)

    loads = [
        pltpu.make_async_copy(src, dst, load_sem.at[n])
        for n, (src, dst) in enumerate(
            [
                (route_e_hbm, route_e),
                (route_w_hbm, route_w),
                (mid_hbm.at[:, lanes(tp)], mid.at[0]),
                (mid_hbm.at[:, lanes(tp2)], mid.at[1]),
                (cot_hbm.at[:, lanes(tp)], cot.at[0]),
                (cot_hbm.at[:, lanes(tp2)], cot.at[1]),
                (gate_hbm, gate_w),
                (up_hbm, up_w),
                (down_hbm, down_w),
                (conv_pre_hbm, conv_pre),
                (conv_taps_hbm, conv_taps),
                (out_proj_hbm, out_proj),
            ]
        )
    ]
    for c in loads:
        c.start()
    for c in loads[0:6]:
        c.wait()

    experts = route_e[...]
    z_rel = experts // X - mz
    z_rel = jnp.where(z_rel < 0, z_rel + Z, z_rel)
    x_rel = experts % X - mx
    x_rel = jnp.where(x_rel < 0, x_rel + X, x_rel)
    turn = jnp.where(2 * z_rel <= Z, jnp.maximum(2 * z_rel - 1, 0), 2 * (Z - z_rel))
    e_rel = turn * X + x_rel
    e_iota = lax.broadcasted_iota(jnp.int32, (S, TOK), 0)
    oh = [e_iota == e_rel[k : k + 1, :] for k in range(2)]
    oh_sum = (oh[0] | oh[1]).astype(F32).astype(BF16)
    before = (
        lax.broadcasted_iota(jnp.int32, (TOK, TOK), 0)
        < lax.broadcasted_iota(jnp.int32, (TOK, TOK), 1)
    ).astype(F32).astype(BF16)
    counts = jnp.dot(oh_sum, before, preferred_element_type=F32)
    main_rows = lax.broadcasted_iota(jnp.int32, (R, TOK), 0)
    ext_rows = lax.broadcasted_iota(jnp.int32, (S, TOK), 0)
    pair_rows = lax.broadcasted_iota(jnp.int32, (2 * S, TOK), 0)
    g_main, g_ext, g_pair = [], [], []
    for k in range(2):
        rank = jnp.sum(jnp.where(oh[k], counts, 0.0), axis=0, keepdims=True).astype(jnp.int32)
        own = e_rel[k : k + 1, :]
        key = jnp.where(rank < MAIN, own * MAIN + rank, -1)
        key_x = jnp.where(rank == MAIN, own, -1)
        g_main.append(main_rows == key)
        g_ext.append(ext_rows == key_x)
        g_pair.append(pair_rows == 2 * key_x + 1)
    w = [route_w[k : k + 1, :] for k in range(2)]
    gm = (g_main[0] | g_main[1]).astype(F32).astype(BF16)
    onehot[...] = gm
    onehot_x[...] = (g_ext[0] | g_ext[1]).astype(F32).astype(BF16)
    mid_c = jnp.concatenate([mid[0], mid[1]], axis=1)
    cot_c = jnp.concatenate([cot[0], cot[1]], axis=1)
    w_main = jnp.sum(
        jnp.where(g_main[0], w[0], 0.0) + jnp.where(g_main[1], w[1], 0.0), axis=1, keepdims=True
    )
    in_rows = jnp.dot(gm, mid_c, preferred_element_type=F32).astype(BF16)
    seed_rows = (w_main * jnp.dot(gm, cot_c, preferred_element_type=F32)).astype(BF16)
    w_pair = jnp.sum(
        jnp.where(g_pair[0], w[0], 0.0) + jnp.where(g_pair[1], w[1], 0.0), axis=1, keepdims=True
    )
    g_odd = (g_pair[0] | g_pair[1]).astype(F32).astype(BF16)
    pair_even = lax.broadcasted_iota(jnp.int32, (2 * S, S), 0) == 2 * lax.broadcasted_iota(
        jnp.int32, (2 * S, S), 1
    )
    g_even = jnp.dot(
        pair_even.astype(F32).astype(BF16), onehot_x[...], preferred_element_type=F32
    ).astype(BF16)
    pair_val = (
        jnp.dot(g_even, mid_c, preferred_element_type=F32)
        + w_pair * jnp.dot(g_odd, cot_c, preferred_element_type=F32)
    ).astype(BF16)
    for m in range(2):
        part = slice(m * LANES, (m + 1) * LANES)
        send_main[m, :, 0:MAIN, :] = in_rows[:, part].reshape(S, MAIN, LANES)
        send_main[m, :, MAIN : 2 * MAIN, :] = seed_rows[:, part].reshape(S, MAIN, LANES)
        for s in range(S):
            send_ext[m, s] = pair_val[2 * s : 2 * s + 2, part]

    pl.semaphore_wait(barrier, S + 2)

    @pl.loop(1, S)
    def _(k):
        dst = apart(k, 1)
        q = k // KQ
        for m in range(2):
            for b, (src, ref) in enumerate(((send_main, rows), (send_ext, ext))):
                copy_to(
                    src.at[m, k],
                    ref.at[mine[m], k],
                    a2a_send.at[m, b],
                    a2a_recv.at[m, b, q],
                    dst,
                    tp,
                ).start()

    for m in range(2):
        rows[mine[m], 0] = send_main[m, 0]
        ext[mine[m], 0] = send_ext[m, 0]

    both = (rows, ext)
    sent = []

    def start_all(copies):
        for c in copies:
            c.start()
        sent.extend(copies)

    def sub(ref, j, q):
        return ref.at[j, pl.ds(q * KQ, KQ)]

    def ag_copies(d, t, m, q, j):
        return [
            copy_to(
                sub(ref, j, q),
                sub(ref, j, q),
                ag_send.at[d, t, m, q, b],
                ag_recv.at[d, t, m, q, b],
                me,
                peers[d],
            )
            for b, ref in enumerate(both)
        ]

    def sib_copies(i, q, j):
        return [
            copy_to(
                sub(ref, j, q), sub(ref, j, q), sib_send.at[i, q, b], sib_recv.at[i, q, b], me, sib
            )
            for b, ref in enumerate(both)
        ]

    def hops(m):
        return G - m

    def near(d, t, m):
        return ((t + 1) if d == 0 else Y - (t + 1)) + m * H

    def slot_of(i):
        return i % Y

    def step_a(q):
        lo = 1 if q == 0 else q * KQ
        n = (q + 1) * KQ - lo
        if n > 0:
            for m in range(2):
                for b, (src, ref) in enumerate(((send_main, rows), (send_ext, ext))):
                    copy_to(
                        src.at[m, pl.ds(lo, n)],
                        ref.at[mine[m], pl.ds(lo, n)],
                        a2a_send.at[m, b],
                        a2a_recv.at[m, b, q],
                        me,
                        sib,
                    ).wait_recv()
        for m in range(2):
            for d in range(2):
                if hops(m) > 0:
                    start_all(ag_copies(d, 0, m, q, mine[m]))
        for m in range(2):
            start_all(sib_copies(m * H, q, mine[m]))

    def arrive(d, t, m, q):
        i = slot_of(near(d, t, m))
        j = chunk(i, core)
        for c in ag_copies(d, t, m, q, j):
            c.wait_recv()
        if t + 1 < hops(m):
            start_all(ag_copies(d, t + 1, m, q, j))
        start_all(sib_copies(i, q, j))

    def step_f(q):
        for m in range(2):
            for d in range(2):
                if hops(m) > 0:
                    arrive(d, 0, m, q)

    def step_e(q):
        for t in range(1, G):
            for m in range(2):
                for d in range(2):
                    if t < hops(m):
                        arrive(d, t, m, q)

    sel_row = lax.broadcasted_iota(jnp.int32, (KQ, 2 * KQ), 0)
    sel_col = lax.broadcasted_iota(jnp.int32, (KQ, 2 * KQ), 1)
    sels = [(sel_col == 2 * sel_row + b).astype(F32).astype(BF16) for b in range(2)]

    def rsib_copy(q):
        return copy_to(
            sib_out.at[q, 1 - core], sib_in.at[q], rsib_send.at[q], rsib_recv.at[q], me, sib
        )

    def step_c(q):
        for i in range(Y):
            for c in sib_copies(i, q, chunk(i, 1 - core)):
                c.wait_recv()
        if q == 0:
            for c in loads[6:9]:
                c.wait()
        for j in range(T):
            for s in range(KQ):
                ext_flat[2 * s : 2 * s + 2, j * LANES : (j + 1) * LANES] = ext[j, q * KQ + s]
        flat = ext_flat[...]
        ext_q = slice(q * KQ, (q + 1) * KQ)
        x_ext = jnp.dot(sels[0], flat, preferred_element_type=F32)
        s_ext = jnp.dot(sels[1], flat, preferred_element_type=F32)
        ext_in[ext_q, :] = x_ext
        ext_seed[ext_q, :] = s_ext
        x = jnp.concatenate(
            [rows[j, q * KQ : (q + 1) * KQ, 0:MAIN, :].reshape(RQ, LANES) for j in range(T)],
            axis=1,
        )
        x = jnp.concatenate([x, x_ext.astype(BF16)], axis=0)
        g = jnp.concatenate(
            [
                rows[j, q * KQ : (q + 1) * KQ, MAIN : 2 * MAIN, :].reshape(RQ, LANES)
                for j in range(T)
            ],
            axis=1,
        )
        g = jnp.concatenate([g, s_ext.astype(BF16)], axis=0)
        w_gu = jnp.concatenate([gate_w[...], up_w[...]], axis=1)
        gate_up = jnp.dot(x, w_gu, preferred_element_type=F32)
        gate_pre = gate_up[:, 0:LANES]
        up_pre = gate_up[:, LANES : 2 * LANES]
        h_grad = lax.dot_general(
            g, down_w[...], (((1,), (1,)), ((), ())), preferred_element_type=F32
        )
        sig = jax.nn.sigmoid(gate_pre)
        act = gate_pre * sig
        hid = (act * up_pre).astype(BF16)
        gate_g = (h_grad * up_pre * (sig * (1.0 + gate_pre * (1.0 - sig)))).astype(BF16)
        pre = jnp.concatenate([gate_g, (h_grad * act).astype(BF16)], axis=1)
        hid_main[q * RQ : (q + 1) * RQ, :] = hid[0:RQ]
        hid_ext[ext_q, :] = hid[RQ:NG].astype(F32)
        pre_main[q * RQ : (q + 1) * RQ, :] = pre[0:RQ]
        pre_ext[ext_q, :] = pre[RQ:NG].astype(F32)

        parts = lax.dot_general(pre, w_gu, (((1,), (1,)), ((), ())), preferred_element_type=F32)
        for j in range(T):
            value = parts[:, j * LANES : (j + 1) * LANES]
            own_part[q, j] = value
            sib_out[q, j % 2, j // 2] = value.astype(BF16)
        start_all([rsib_copy(q)])

    def rs_copy(d, t, q):
        return copy_to(
            ring_out.at[d, t, q],
            ring_in.at[d, t, q],
            rs_send.at[d, t, q],
            rs_recv.at[d, t, q],
            me,
            peers[d],
        )

    def rs_has(d, t, q):
        if t < 0:
            return False
        return t > 0 or q % 2 == d

    def step_b(q, t):
        if t == 0:
            rsib_copy(q).wait_recv()
        if t == H:
            value = own_part[q, tp] + sib_in[q, y].astype(F32)
            for d in range(2):
                if rs_has(d, H - 1, q):
                    rs_copy(d, H - 1, q).wait_recv()
                    value = value + ring_in[d, H - 1, q].astype(F32)
            value = value.astype(BF16)
            back_main[q * KQ : (q + 1) * KQ] = value[0:RQ].reshape(KQ, MAIN, LANES)
            last = value[RQ:NG].astype(F32)
            for s in range(KQ):
                back_ext[q * KQ + s] = last[s : s + 1, :]
            if q == 0:
                home_main[0] = back_main[0]
                home_ext[0] = back_ext[0]

            @pl.loop(max(1, q * KQ), (q + 1) * KQ)
            def _(k):
                dst = apart(k, -1)
                for b, (src, ref) in enumerate(((back_main, home_main), (back_ext, home_ext))):
                    copy_to(
                        src.at[k], ref.at[k], ret_send.at[b], ret_recv.at[b], dst, tp
                    ).start()

            return
        dist = H - t
        for d in range(2):
            if not rs_has(d, t, q):
                continue
            o = dist if d == 0 else Y - dist
            to = lax.rem(y + o, Y)
            value = own_part[q, 2 * to + core] + sib_in[q, to].astype(F32)
            if rs_has(d, t - 1, q):
                rs_copy(d, t - 1, q).wait_recv()
                value = value + ring_in[d, t - 1, q].astype(F32)
            ring_out[d, t, q] = value.astype(BF16)
            start_all([rs_copy(d, t, q)])

    def weight_grads(j):
        x = jnp.concatenate(
            [rows[j, :, 0:MAIN, :].reshape(R, LANES), ext_in[:, lanes(j)].astype(BF16)], axis=0
        )
        g = jnp.concatenate(
            [
                rows[j, :, MAIN : 2 * MAIN, :].reshape(R, LANES),
                ext_seed[:, lanes(j)].astype(BF16),
            ],
            axis=0,
        )
        pre = jnp.concatenate([pre_main[...], pre_ext[...].astype(BF16)], axis=0)
        hid = jnp.concatenate([hid_main[...], hid_ext[...].astype(BF16)], axis=0)
        both_g = lax.dot_general(
            x, pre, (((0,), (0,)), ((), ())), preferred_element_type=F32
        ).astype(BF16)
        grad_gate[lanes(j), :] = both_g[:, 0:LANES]
        grad_up[lanes(j), :] = both_g[:, LANES : 2 * LANES]
        grad_down[:, lanes(j)] = lax.dot_general(
            hid, g, (((0,), (0,)), ((), ())), preferred_element_type=F32
        ).astype(BF16)

    reached = [-1] * NQ
    ready = [0]

    def round_b():
        for q in range(ready[0]):
            if reached[q] < H:
                reached[q] += 1
                step_b(q, reached[q])

    step_a(0)
    for q in range(1, NQ + 3):
        if q < NQ:
            step_a(q)
        if 0 <= q - 1 < NQ:
            step_f(q - 1)
        if 0 <= q - 2 < NQ:
            step_e(q - 2)
        if 0 <= q - 3 < NQ:
            step_c(q - 3)
            ready[0] += 1
    done = 0
    for s in range(H + 1):
        round_b()
        stop = T * (s + 1) // (H + 1)

        @pl.loop(done, stop)
        def _(j):
            weight_grads(j)

        done = stop

    for c in loads[9:12]:
        c.wait()
    pre = conv_pre[...].astype(F32)
    pre_sig = jax.nn.sigmoid(pre)
    activated = (pre * pre_sig).astype(BF16)
    eye = (
        lax.broadcasted_iota(jnp.int32, (KERNEL, KERNEL), 0)
        == lax.broadcasted_iota(jnp.int32, (KERNEL, KERNEL), 1)
    ).astype(F32).astype(BF16)
    taps = lax.dot_general(
        conv_taps[...], eye, (((0,), (0,)), ((), ())), preferred_element_type=F32
    )
    for b, (src, ref) in enumerate(((back_main, home_main), (back_ext, home_ext))):
        copy_to(
            src.at[pl.ds(1, S - 1)],
            ref.at[pl.ds(1, S - 1)],
            ret_send.at[b],
            ret_recv.at[b],
            me,
            sib,
        ).wait()
    home_x = jnp.concatenate([home_ext[s] for s in range(S)], axis=0).astype(BF16)
    moe = lax.dot_general(
        onehot[...],
        home_main[...].reshape(R, LANES),
        (((0,), (0,)), ((), ())),
        preferred_element_type=F32,
    ) + lax.dot_general(
        onehot_x[...], home_x, (((0,), (0,)), ((), ())), preferred_element_type=F32
    )
    gathered[tp] = (cot[0].astype(F32) + moe).astype(BF16)

    TH = TOK // 2

    def mg_copy(d, t, h, j):
        part = gathered.at[j, pl.ds(h * TH, TH)]
        return copy_to(part, part, mg_send.at[d, t, h], mg_recv.at[d, t, h], me, peers[d])

    def mgs_copy(i, h, j):
        part = gathered.at[j, pl.ds(h * TH, TH)]
        return copy_to(part, part, mgs_send.at[i, h], mgs_recv.at[i, h], me, sib)

    def mg_carries(d, t, h):
        if t + 1 < H:
            return True
        if t + 1 > H:
            return False
        return h == d

    mixed[...] = jnp.zeros_like(mixed)
    units = proj_out.shape[0] // S
    low = lax.broadcasted_iota(jnp.int32, (CC // 2, LANES), 1) < LANES // 2

    def use_mid(i):
        for h in range(2):
            mgs_copy(i, h, chunk(i, 1 - core)).wait_recv()
        j0 = chunk(i, 0)
        g = jnp.concatenate([gathered[j0], gathered[j0 + 1]], axis=1)
        mixed[...] += lax.dot_general(
            out_proj[:, lanes(j0, 2)], g, (((1,), (1,)), ((), ())), preferred_element_type=F32
        )
        part = jnp.dot(activated, g, preferred_element_type=F32)
        for p in range(2):
            top = part[0 : CC // 2, p * LANES : (p + 1) * LANES]
            low_c = part[CC // 2 : CC, p * LANES : (p + 1) * LANES]
            proj_out[2 * (j0 + p)] = jnp.where(
                low, top, pltpu.roll(low_c, LANES // 2, 1)
            ).astype(BF16)
            proj_out[2 * (j0 + p) + 1] = jnp.where(
                low, pltpu.roll(top, LANES // 2, 1), low_c
            ).astype(BF16)
        for p in range(4):
            u = 2 * j0 + p
            dst = u // units
            k = lax.rem(dst - me + S, S)

            @pl.when(k > 0)
            def _():
                copy_to(
                    proj_out.at[u],
                    proj_in.at[k * units + lax.rem(u, units)],
                    proj_send.at[0],
                    proj_recv.at[0],
                    dst,
                    tp,
                ).start()

    for h in range(2):
        for d in range(2):
            if mg_carries(d, 0, h):
                start_all([mg_copy(d, 0, h, tp)])
        start_all([mgs_copy(0, h, tp)])
    use_mid(0)
    for t in range(H):
        for h in range(2):
            for d in range(2):
                if not mg_carries(d, t, h):
                    continue
                i = t + 1 if d == 0 else Y - (t + 1)
                j = chunk(i, core)
                mg_copy(d, t, h, j).wait_recv()
                if mg_carries(d, t + 1, h):
                    start_all([mg_copy(d, t + 1, h, j)])
                start_all([mgs_copy(i, h, j)])
        if t + 1 < H:
            use_mid(t + 1)
            use_mid(Y - (t + 1))
        else:
            use_mid(H)

    conv_grad = (mixed[...] * (pre_sig * (1.0 + pre * (1.0 - pre_sig)))).astype(BF16)
    halo_out[...] = conv_grad[:, 0:HW]
    halo = copy_to(
        halo_out, halo_in, halo_send.at[0], halo_recv.at[0], lax.rem(me + S - 1, S), tp
    )
    start_all([halo])
    for m in range(2):
        for b, (src, ref) in enumerate(((send_main, rows), (send_ext, ext))):
            copy_to(
                src.at[m, pl.ds(1, S - 1)],
                ref.at[mine[m], pl.ds(1, S - 1)],
                a2a_send.at[m, b],
                a2a_recv.at[m, b, 0],
                me,
                sib,
            ).wait_send()
    for c in sent[:-1]:
        c.wait_send()
    halo.wait_recv()
    beyond = jnp.where(me == S - 1, 0.0, halo_in[...].astype(F32))
    extended = jnp.concatenate([conv_grad.astype(F32), beyond], axis=1)
    total = taps[:, 0:1] * extended[:, 0:TOK]
    for lag in range(1, KERNEL):
        shifted = pltpu.roll(extended, TOK + HW - lag, 1)
        total = total + taps[:, lag : lag + 1] * shifted[:, 0:TOK]
    conv_in_grad[...] = total

    copy_to(
        proj_out.at[pl.ds(units, (S - 1) * units)],
        proj_in.at[pl.ds(units, (S - 1) * units)],
        proj_send.at[0],
        proj_recv.at[0],
        me,
        sib,
    ).wait()
    for u in range(units):
        z = proj_out[me * units + u].astype(F32)
        for k in range(1, S):
            z = z + proj_in[k * units + u].astype(F32)
        tall = jnp.concatenate([z, pltpu.roll(z, LANES // 2, 1)], axis=0)
        grad_proj[u * (LANES // 2) : (u + 1) * (LANES // 2), :] = tall.T[0 : LANES // 2, :]
    halo.wait_send()


def moe_call(S, T, *args):
    Y = T // 2
    H = Y // 2
    G = max(1, Y // 4)
    TOK, D = args[2].shape
    CC = args[7].shape[0]
    NQ = min(4, S)
    KQ = S // NQ
    R = S * MAIN
    NG = KQ * MAIN + KQ
    HW = min(LANES, TOK)
    vmem = pl.BlockSpec(memory_space=pltpu.VMEM)
    hbm = pl.BlockSpec(memory_space=pltpu.HBM)
    dma = pltpu.SemaphoreType.DMA
    scratch = [
        pltpu.VMEM(args[0].shape, jnp.int32),
        pltpu.VMEM(args[1].shape, F32),
        pltpu.VMEM((2, TOK, LANES), BF16),
        pltpu.VMEM((2, TOK, LANES), BF16),
        pltpu.VMEM((D, LANES), BF16),
        pltpu.VMEM((D, LANES), BF16),
        pltpu.VMEM((LANES, D), BF16),
        pltpu.VMEM(args[7].shape, BF16),
        pltpu.VMEM(args[8].shape, BF16),
        pltpu.VMEM(args[9].shape, BF16),
        dma((12,)),
        pltpu.VMEM((2, S, 2 * MAIN, LANES), BF16),
        pltpu.VMEM((2, S, 2, LANES), BF16),
        pltpu.VMEM((T, S, 2 * MAIN, LANES), BF16),
        pltpu.VMEM((T, S, 2, LANES), BF16),
        pltpu.VMEM((2 * KQ, D), BF16),
        pltpu.VMEM((S, D), F32),
        pltpu.VMEM((S, D), F32),
        pltpu.VMEM((R, TOK), BF16),
        pltpu.VMEM((S, TOK), BF16),
        pltpu.VMEM((R, LANES), BF16),
        pltpu.VMEM((S, LANES), F32),
        pltpu.VMEM((R, 2 * LANES), BF16),
        pltpu.VMEM((S, 2 * LANES), F32),
        pltpu.VMEM((NQ, 2, Y, NG, LANES), BF16),
        pltpu.VMEM((NQ, Y, NG, LANES), BF16),
        pltpu.VMEM((NQ, T, NG, LANES), F32),
        pltpu.VMEM((2, H, NQ, NG, LANES), BF16),
        pltpu.VMEM((2, H, NQ, NG, LANES), BF16),
        pltpu.VMEM((S, MAIN, LANES), BF16),
        pltpu.VMEM((S, 1, LANES), F32),
        pltpu.VMEM((S, MAIN, LANES), BF16),
        pltpu.VMEM((S, 1, LANES), F32),
        pltpu.VMEM((T, TOK, LANES), BF16),
        pltpu.VMEM((CC, TOK), F32),
        pltpu.VMEM((2 * T, CC // 2, LANES), BF16),
        pltpu.VMEM((2 * T, CC // 2, LANES), BF16),
        pltpu.VMEM((CC, HW), BF16),
        pltpu.VMEM((CC, HW), BF16),
        dma((2, 2)),
        dma((2, 2, NQ)),
        dma((2, G, 2, NQ, 2)),
        dma((2, G, 2, NQ, 2)),
        dma((Y, NQ, 2)),
        dma((Y, NQ, 2)),
        dma((NQ,)),
        dma((NQ,)),
        dma((2, H, NQ)),
        dma((2, H, NQ)),
        dma((2,)),
        dma((2,)),
        dma((2, H, 2)),
        dma((2, H, 2)),
        dma((Y, 2)),
        dma((Y, 2)),
        dma((1,)),
        dma((1,)),
        dma((1,)),
        dma((1,)),
    ]
    return pl.pallas_call(
        functools.partial(moe_kernel, S, T, NQ),
        out_shape=(
            jax.ShapeDtypeStruct((D, LANES), BF16),
            jax.ShapeDtypeStruct((D, LANES), BF16),
            jax.ShapeDtypeStruct((LANES, D), BF16),
            jax.ShapeDtypeStruct((D // S, CC), F32),
            jax.ShapeDtypeStruct((CC, TOK), F32),
        ),
        in_specs=[hbm] * len(args),
        out_specs=(vmem,) * 5,
        scratch_shapes=scratch,
        compiler_params=pltpu.CompilerParams(
            collective_id=0, has_side_effects=True, vmem_limit_bytes=36 * 1024 * 1024
        ),
    )(*[pltpu.with_memory_space_constraint(a, pltpu.HBM) for a in args])


def body(
    S,
    T,
    mid_state,
    conv_pre,
    conv_taps,
    out_proj,
    route_expert,
    route_weight,
    gate_w,
    up_w,
    down_w,
    cotangent,
):
    grad_gate, grad_up, grad_down, grad_proj, conv_in_grad = moe_call(
        S,
        T,
        route_expert.T,
        route_weight.T,
        mid_state,
        cotangent,
        gate_w[0],
        up_w[0],
        down_w[0],
        conv_pre.T,
        conv_taps,
        out_proj,
    )
    return (grad_gate[None], grad_up[None], grad_down[None], grad_proj, conv_in_grad.T)


def solution(mesh):
    placed = (
        P("sp", None),
        P("sp", "tp"),
        P(None, "tp"),
        P("tp", None),
        P("sp", None),
        P("sp", None),
        P("sp", None, "tp"),
        P("sp", None, "tp"),
        P("sp", "tp", None),
        P("sp", None),
    )
    return jax.shard_map(
        functools.partial(body, mesh.shape["sp"], mesh.shape["tp"]),
        mesh=mesh,
        in_specs=placed,
        out_specs=(
            P("sp", None, "tp"),
            P("sp", None, "tp"),
            P("sp", "tp", None),
            P("sp", "tp"),
            P("sp", "tp"),
        ),
        check_vma=False,
    )
```

```python
import functools

import jax
import jax.numpy as jnp
from jax import lax
from jax.experimental import pallas as pl
from jax.experimental.pallas import tpu as pltpu
from jax.sharding import PartitionSpec as P

KERNEL = 31
LANES = 128
MAIN = 16
MESH = pl.DeviceIdType.MESH
F32 = jnp.float32
BF16 = jnp.bfloat16


def copy_to(src, dst, send, recv, sp, tp):
    return pltpu.make_async_remote_copy(
        src_ref=src,
        dst_ref=dst,
        send_sem=send,
        recv_sem=recv,
        device_id=(sp, tp),
        device_id_type=MESH,
    )


def moe_kernel(
    S,
    T,
    NQ,
    route_e_hbm,
    route_w_hbm,
    mid_hbm,
    cot_hbm,
    gate_hbm,
    up_hbm,
    down_hbm,
    conv_pre_hbm,
    conv_taps_hbm,
    out_proj_hbm,
    grad_gate,
    grad_up,
    grad_down,
    grad_proj,
    conv_in_grad,
    route_e,
    route_w,
    mid,
    cot,
    gate_w,
    up_w,
    down_w,
    conv_pre,
    conv_taps,
    out_proj,
    load_sem,
    send_main,
    send_ext,
    rows,
    ext,
    ext_flat,
    ext_in,
    ext_seed,
    onehot,
    onehot_x,
    hid_main,
    hid_ext,
    pre_main,
    pre_ext,
    sib_out,
    sib_in,
    own_part,
    ring_out,
    ring_in,
    back_main,
    back_ext,
    home_main,
    home_ext,
    gathered,
    mixed,
    proj_out,
    proj_in,
    halo_out,
    halo_in,
    a2a_send,
    a2a_recv,
    ag_send,
    ag_recv,
    sib_send,
    sib_recv,
    rsib_send,
    rsib_recv,
    rs_send,
    rs_recv,
    ret_send,
    ret_recv,
    mg_send,
    mg_recv,
    mgs_send,
    mgs_recv,
    proj_send,
    proj_recv,
    halo_send,
    halo_recv,
):
    Y = T // 2
    H = Y // 2
    G = Y // 4
    KQ = S // NQ
    R = S * MAIN
    RQ = KQ * MAIN
    NG = RQ + KQ
    TOK = mid.shape[1]
    CC = conv_pre.shape[0]
    HW = halo_out.shape[1]
    me = lax.axis_index("sp")
    tp = lax.axis_index("tp")
    y = tp // 2
    core = tp % 2
    sib = tp + 1 - 2 * core
    right = lax.rem(tp + 2, T)
    left = lax.rem(tp + T - 2, T)
    peers = (right, left)
    peers2 = (lax.rem(tp + 4, T), lax.rem(tp + T - 4 + T, T))
    tp2 = lax.rem(tp + H * 2, T)
    mine = (tp, tp2)

    X = 4 if S >= 16 else 1
    Z = S // X
    mz = me // X
    mx = me % X

    def apart(b, sign):
        c = b // X
        zo = jnp.where(c % 2 == 1, (c + 1) // 2, -(c // 2))
        return lax.rem(mz + sign * zo + Z, Z) * X + lax.rem(mx + sign * (b % X) + X, X)

    def chunk(i, parity):
        return 2 * lax.rem(y - i + 2 * Y, Y) + parity

    def lanes(j, width=1):
        return pl.ds(pl.multiple_of(j * LANES, LANES * width), LANES * width)

    barrier = pltpu.get_barrier_semaphore()

    @pl.loop(1, S)
    def _(k):
        pl.semaphore_signal(
            barrier, inc=1, device_id=(apart(k, 1), tp), device_id_type=MESH
        )

    for peer in (left, right, sib) + (peers2 if H > 1 else ()):
        pl.semaphore_signal(barrier, inc=1, device_id=(me, peer), device_id_type=MESH)

    loads = [
        pltpu.make_async_copy(src, dst, load_sem.at[n])
        for n, (src, dst) in enumerate(
            [
                (route_e_hbm, route_e),
                (route_w_hbm, route_w),
                (mid_hbm.at[:, lanes(tp)], mid.at[0]),
                (mid_hbm.at[:, lanes(tp2)], mid.at[1]),
                (cot_hbm.at[:, lanes(tp)], cot.at[0]),
                (cot_hbm.at[:, lanes(tp2)], cot.at[1]),
                (gate_hbm, gate_w),
                (up_hbm, up_w),
                (down_hbm, down_w),
                (conv_pre_hbm, conv_pre),
                (conv_taps_hbm, conv_taps),
                (out_proj_hbm, out_proj),
            ]
        )
    ]
    for c in loads:
        c.start()
    for c in loads[0:6]:
        c.wait()

    experts = route_e[...]
    z_rel = experts // X - mz
    z_rel = jnp.where(z_rel < 0, z_rel + Z, z_rel)
    x_rel = experts % X - mx
    x_rel = jnp.where(x_rel < 0, x_rel + X, x_rel)
    turn = jnp.where(2 * z_rel <= Z, jnp.maximum(2 * z_rel - 1, 0), 2 * (Z - z_rel))
    e_rel = turn * X + x_rel
    e_iota = lax.broadcasted_iota(jnp.int32, (S, TOK), 0)
    oh = [e_iota == e_rel[k : k + 1, :] for k in range(2)]
    oh_sum = (oh[0] | oh[1]).astype(F32).astype(BF16)
    before = (
        lax.broadcasted_iota(jnp.int32, (TOK, TOK), 0)
        < lax.broadcasted_iota(jnp.int32, (TOK, TOK), 1)
    ).astype(F32).astype(BF16)
    counts = jnp.dot(oh_sum, before, preferred_element_type=F32)
    main_rows = lax.broadcasted_iota(jnp.int32, (R, TOK), 0)
    ext_rows = lax.broadcasted_iota(jnp.int32, (S, TOK), 0)
    pair_rows = lax.broadcasted_iota(jnp.int32, (2 * S, TOK), 0)
    g_main, g_ext, g_pair = [], [], []
    for k in range(2):
        rank = jnp.sum(jnp.where(oh[k], counts, 0.0), axis=0, keepdims=True).astype(jnp.int32)
        own = e_rel[k : k + 1, :]
        key = jnp.where(rank < MAIN, own * MAIN + rank, -1)
        key_x = jnp.where(rank == MAIN, own, -1)
        g_main.append(main_rows == key)
        g_ext.append(ext_rows == key_x)
        g_pair.append(pair_rows == 2 * key_x + 1)
    w = [route_w[k : k + 1, :] for k in range(2)]
    gm = (g_main[0] | g_main[1]).astype(F32).astype(BF16)
    onehot[...] = gm
    onehot_x[...] = (g_ext[0] | g_ext[1]).astype(F32).astype(BF16)
    mid_c = jnp.concatenate([mid[0], mid[1]], axis=1)
    cot_c = jnp.concatenate([cot[0], cot[1]], axis=1)
    w_main = jnp.sum(
        jnp.where(g_main[0], w[0], 0.0) + jnp.where(g_main[1], w[1], 0.0), axis=1, keepdims=True
    )
    in_rows = jnp.dot(gm, mid_c, preferred_element_type=F32).astype(BF16)
    seed_rows = (w_main * jnp.dot(gm, cot_c, preferred_element_type=F32)).astype(BF16)
    w_pair = jnp.sum(
        jnp.where(g_pair[0], w[0], 0.0) + jnp.where(g_pair[1], w[1], 0.0), axis=1, keepdims=True
    )
    g_odd = (g_pair[0] | g_pair[1]).astype(F32).astype(BF16)
    pair_even = lax.broadcasted_iota(jnp.int32, (2 * S, S), 0) == 2 * lax.broadcasted_iota(
        jnp.int32, (2 * S, S), 1
    )
    g_even = jnp.dot(
        pair_even.astype(F32).astype(BF16), onehot_x[...], preferred_element_type=F32
    ).astype(BF16)
    pair_val = (
        jnp.dot(g_even, mid_c, preferred_element_type=F32)
        + w_pair * jnp.dot(g_odd, cot_c, preferred_element_type=F32)
    ).astype(BF16)
    for m in range(2):
        part = slice(m * LANES, (m + 1) * LANES)
        send_main[m, :, 0:MAIN, :] = in_rows[:, part].reshape(S, MAIN, LANES)
        send_main[m, :, MAIN : 2 * MAIN, :] = seed_rows[:, part].reshape(S, MAIN, LANES)
        for s in range(S):
            send_ext[m, s] = pair_val[2 * s : 2 * s + 2, part]

    pl.semaphore_wait(barrier, S + 2 + (2 if H > 1 else 0))

    @pl.loop(1, S)
    def _(k):
        dst = apart(k, 1)
        q = k // KQ
        for m in range(2):
            for b, (src, ref) in enumerate(((send_main, rows), (send_ext, ext))):
                copy_to(
                    src.at[m, k],
                    ref.at[mine[m], k],
                    a2a_send.at[m, b],
                    a2a_recv.at[m, b, q],
                    dst,
                    tp,
                ).start()

    for m in range(2):
        rows[mine[m], 0] = send_main[m, 0]
        ext[mine[m], 0] = send_ext[m, 0]

    both = (rows, ext)
    sent = []

    def start_all(copies):
        for c in copies:
            c.start()
        sent.extend(copies)

    def sub(ref, j, q):
        return ref.at[j, pl.ds(q * KQ, KQ)]

    def ag_copies(d, t, m, q, j):
        return [
            copy_to(
                sub(ref, j, q),
                sub(ref, j, q),
                ag_send.at[d, t, m, q, b],
                ag_recv.at[d, t, m, q, b],
                me,
                peers[d],
            )
            for b, ref in enumerate(both)
        ]

    def sib_copies(i, q, j):
        return [
            copy_to(
                sub(ref, j, q), sub(ref, j, q), sib_send.at[i, q, b], sib_recv.at[i, q, b], me, sib
            )
            for b, ref in enumerate(both)
        ]

    def hops(m):
        return G - m

    def near(d, t, m):
        return ((t + 1) if d == 0 else Y - (t + 1)) + m * H

    def slot_of(i):
        return i % Y

    def step_a(q):
        lo = 1 if q == 0 else q * KQ
        n = (q + 1) * KQ - lo
        if n > 0:
            for m in range(2):
                for b, (src, ref) in enumerate(((send_main, rows), (send_ext, ext))):
                    copy_to(
                        src.at[m, pl.ds(lo, n)],
                        ref.at[mine[m], pl.ds(lo, n)],
                        a2a_send.at[m, b],
                        a2a_recv.at[m, b, q],
                        me,
                        sib,
                    ).wait_recv()
        for m in range(2):
            for d in range(2):
                if hops(m) > 0:
                    start_all(ag_copies(d, 0, m, q, mine[m]))
        for m in range(2):
            start_all(sib_copies(m * H, q, mine[m]))

    def arrive(d, t, m, q):
        i = slot_of(near(d, t, m))
        j = chunk(i, core)
        for c in ag_copies(d, t, m, q, j):
            c.wait_recv()
        if t + 1 < hops(m):
            start_all(ag_copies(d, t + 1, m, q, j))
        start_all(sib_copies(i, q, j))

    def step_f(q):
        for m in range(2):
            for d in range(2):
                if hops(m) > 0:
                    arrive(d, 0, m, q)

    def step_e(q):
        for t in range(1, G):
            for m in range(2):
                for d in range(2):
                    if t < hops(m):
                        arrive(d, t, m, q)

    sel_row = lax.broadcasted_iota(jnp.int32, (KQ, 2 * KQ), 0)
    sel_col = lax.broadcasted_iota(jnp.int32, (KQ, 2 * KQ), 1)
    sels = [(sel_col == 2 * sel_row + b).astype(F32).astype(BF16) for b in range(2)]

    def rsib_copy(q):
        return copy_to(
            sib_out.at[q, 1 - core], sib_in.at[q], rsib_send.at[q], rsib_recv.at[q], me, sib
        )

    def step_c(q):
        for i in range(Y):
            for c in sib_copies(i, q, chunk(i, 1 - core)):
                c.wait_recv()
        if q == 0:
            for c in loads[6:9]:
                c.wait()
        for j in range(T):
            for s in range(KQ):
                ext_flat[2 * s : 2 * s + 2, j * LANES : (j + 1) * LANES] = ext[j, q * KQ + s]
        flat = ext_flat[...]
        ext_q = slice(q * KQ, (q + 1) * KQ)
        x_ext = jnp.dot(sels[0], flat, preferred_element_type=F32)
        s_ext = jnp.dot(sels[1], flat, preferred_element_type=F32)
        ext_in[ext_q, :] = x_ext
        ext_seed[ext_q, :] = s_ext
        x = jnp.concatenate(
            [rows[j, q * KQ : (q + 1) * KQ, 0:MAIN, :].reshape(RQ, LANES) for j in range(T)],
            axis=1,
        )
        x = jnp.concatenate([x, x_ext.astype(BF16)], axis=0)
        g = jnp.concatenate(
            [
                rows[j, q * KQ : (q + 1) * KQ, MAIN : 2 * MAIN, :].reshape(RQ, LANES)
                for j in range(T)
            ],
            axis=1,
        )
        g = jnp.concatenate([g, s_ext.astype(BF16)], axis=0)
        w_gu = jnp.concatenate([gate_w[...], up_w[...]], axis=1)
        gate_up = jnp.dot(x, w_gu, preferred_element_type=F32)
        gate_pre = gate_up[:, 0:LANES]
        up_pre = gate_up[:, LANES : 2 * LANES]
        h_grad = lax.dot_general(
            g, down_w[...], (((1,), (1,)), ((), ())), preferred_element_type=F32
        )
        sig = jax.nn.sigmoid(gate_pre)
        act = gate_pre * sig
        hid = (act * up_pre).astype(BF16)
        gate_g = (h_grad * up_pre * (sig * (1.0 + gate_pre * (1.0 - sig)))).astype(BF16)
        pre = jnp.concatenate([gate_g, (h_grad * act).astype(BF16)], axis=1)
        hid_main[q * RQ : (q + 1) * RQ, :] = hid[0:RQ]
        hid_ext[ext_q, :] = hid[RQ:NG].astype(F32)
        pre_main[q * RQ : (q + 1) * RQ, :] = pre[0:RQ]
        pre_ext[ext_q, :] = pre[RQ:NG].astype(F32)

        parts = lax.dot_general(pre, w_gu, (((1,), (1,)), ((), ())), preferred_element_type=F32)
        for j in range(T):
            value = parts[:, j * LANES : (j + 1) * LANES]
            own_part[q, j] = value
            sib_out[q, j % 2, j // 2] = value.astype(BF16)
        start_all([rsib_copy(q)])

    def rs_copy(d, t, q):
        return copy_to(
            ring_out.at[d, t, q],
            ring_in.at[d, t, q],
            rs_send.at[d, t, q],
            rs_recv.at[d, t, q],
            me,
            peers[d],
        )

    def rs_has(d, t, q):
        if t < 0:
            return False
        return t > 0 or q % 2 == d

    def step_b(q, t):
        if t == 0:
            rsib_copy(q).wait_recv()
        if t == H:
            value = own_part[q, tp] + sib_in[q, y].astype(F32)
            for d in range(2):
                if rs_has(d, H - 1, q):
                    rs_copy(d, H - 1, q).wait_recv()
                    value = value + ring_in[d, H - 1, q].astype(F32)
            value = value.astype(BF16)
            back_main[q * KQ : (q + 1) * KQ] = value[0:RQ].reshape(KQ, MAIN, LANES)
            last = value[RQ:NG].astype(F32)
            for s in range(KQ):
                back_ext[q * KQ + s] = last[s : s + 1, :]
            if q == 0:
                home_main[0] = back_main[0]
                home_ext[0] = back_ext[0]

            @pl.loop(max(1, q * KQ), (q + 1) * KQ)
            def _(k):
                dst = apart(k, -1)
                for b, (src, ref) in enumerate(((back_main, home_main), (back_ext, home_ext))):
                    copy_to(
                        src.at[k], ref.at[k], ret_send.at[b], ret_recv.at[b], dst, tp
                    ).start()

            return
        dist = H - t
        for d in range(2):
            if not rs_has(d, t, q):
                continue
            o = dist if d == 0 else Y - dist
            to = lax.rem(y + o, Y)
            value = own_part[q, 2 * to + core] + sib_in[q, to].astype(F32)
            if rs_has(d, t - 1, q):
                rs_copy(d, t - 1, q).wait_recv()
                value = value + ring_in[d, t - 1, q].astype(F32)
            ring_out[d, t, q] = value.astype(BF16)
            start_all([rs_copy(d, t, q)])

    def weight_grads(j):
        x = jnp.concatenate(
            [rows[j, :, 0:MAIN, :].reshape(R, LANES), ext_in[:, lanes(j)].astype(BF16)], axis=0
        )
        g = jnp.concatenate(
            [
                rows[j, :, MAIN : 2 * MAIN, :].reshape(R, LANES),
                ext_seed[:, lanes(j)].astype(BF16),
            ],
            axis=0,
        )
        pre = jnp.concatenate([pre_main[...], pre_ext[...].astype(BF16)], axis=0)
        hid = jnp.concatenate([hid_main[...], hid_ext[...].astype(BF16)], axis=0)
        both_g = lax.dot_general(
            x, pre, (((0,), (0,)), ((), ())), preferred_element_type=F32
        ).astype(BF16)
        grad_gate[lanes(j), :] = both_g[:, 0:LANES]
        grad_up[lanes(j), :] = both_g[:, LANES : 2 * LANES]
        grad_down[:, lanes(j)] = lax.dot_general(
            hid, g, (((0,), (0,)), ((), ())), preferred_element_type=F32
        ).astype(BF16)

    reached = [-1] * NQ
    ready = [0]

    def round_b():
        for q in range(ready[0]):
            if reached[q] < H:
                reached[q] += 1
                step_b(q, reached[q])

    step_a(0)
    for q in range(1, NQ + 3):
        if q < NQ:
            step_a(q)
        if 0 <= q - 1 < NQ:
            step_f(q - 1)
        if 0 <= q - 2 < NQ:
            step_e(q - 2)
        if 0 <= q - 3 < NQ:
            step_c(q - 3)
            ready[0] += 1
    done = 0
    for s in range(H + 1):
        round_b()
        stop = T * (s + 1) // (H + 1)

        @pl.loop(done, stop)
        def _(j):
            weight_grads(j)

        done = stop

    for c in loads[9:12]:
        c.wait()
    pre = conv_pre[...].astype(F32)
    pre_sig = jax.nn.sigmoid(pre)
    activated = (pre * pre_sig).astype(BF16)
    eye = (
        lax.broadcasted_iota(jnp.int32, (KERNEL, KERNEL), 0)
        == lax.broadcasted_iota(jnp.int32, (KERNEL, KERNEL), 1)
    ).astype(F32).astype(BF16)
    taps = lax.dot_general(
        conv_taps[...], eye, (((0,), (0,)), ((), ())), preferred_element_type=F32
    )
    for b, (src, ref) in enumerate(((back_main, home_main), (back_ext, home_ext))):
        copy_to(
            src.at[pl.ds(1, S - 1)],
            ref.at[pl.ds(1, S - 1)],
            ret_send.at[b],
            ret_recv.at[b],
            me,
            sib,
        ).wait()
    home_x = jnp.concatenate([home_ext[s] for s in range(S)], axis=0).astype(BF16)
    moe = lax.dot_general(
        onehot[...],
        home_main[...].reshape(R, LANES),
        (((0,), (0,)), ((), ())),
        preferred_element_type=F32,
    ) + lax.dot_general(
        onehot_x[...], home_x, (((0,), (0,)), ((), ())), preferred_element_type=F32
    )
    gathered[tp] = (cot[0].astype(F32) + moe).astype(BF16)

    TH = TOK // 2

    def mg_copy(d, t, h, j, hop):
        part = gathered.at[j, pl.ds(h * TH, TH)]
        peer = peers[d] if hop == 1 else peers2[d]
        return copy_to(part, part, mg_send.at[d, t, h], mg_recv.at[d, t, h], me, peer)

    def mgs_copy(i, h, j):
        part = gathered.at[j, pl.ds(h * TH, TH)]
        return copy_to(part, part, mgs_send.at[i, h], mgs_recv.at[i, h], me, sib)

    def mg_carries(d, t, h):
        if t + 1 < H:
            return True
        if t + 1 > H:
            return False
        return h == d

    mixed[...] = jnp.zeros_like(mixed)
    units = proj_out.shape[0] // S
    low = lax.broadcasted_iota(jnp.int32, (CC // 2, LANES), 1) < LANES // 2

    def use_mid(i):
        for h in range(2):
            mgs_copy(i, h, chunk(i, 1 - core)).wait_recv()
        j0 = chunk(i, 0)
        g = jnp.concatenate([gathered[j0], gathered[j0 + 1]], axis=1)
        mixed[...] += lax.dot_general(
            out_proj[:, lanes(j0, 2)], g, (((1,), (1,)), ((), ())), preferred_element_type=F32
        )
        part = jnp.dot(activated, g, preferred_element_type=F32)
        for p in range(2):
            top = part[0 : CC // 2, p * LANES : (p + 1) * LANES]
            low_c = part[CC // 2 : CC, p * LANES : (p + 1) * LANES]
            proj_out[2 * (j0 + p)] = jnp.where(
                low, top, pltpu.roll(low_c, LANES // 2, 1)
            ).astype(BF16)
            proj_out[2 * (j0 + p) + 1] = jnp.where(
                low, pltpu.roll(top, LANES // 2, 1), low_c
            ).astype(BF16)
        for p in range(4):
            u = 2 * j0 + p
            dst = u // units
            k = lax.rem(dst - me + S, S)

            @pl.when(k > 0)
            def _():
                copy_to(
                    proj_out.at[u],
                    proj_in.at[k * units + lax.rem(u, units)],
                    proj_send.at[0],
                    proj_recv.at[0],
                    dst,
                    tp,
                ).start()

    for hop in range(1, 3):
        for h in range(2):
            for d in range(2):
                if mg_carries(d, hop - 1, h):
                    start_all([mg_copy(d, hop - 1, h, tp, hop)])
            if hop == 1:
                start_all([mgs_copy(0, h, tp)])
    use_mid(0)
    for t in range(H):
        for h in range(2):
            for d in range(2):
                if not mg_carries(d, t, h):
                    continue
                i = t + 1 if d == 0 else Y - (t + 1)
                j = chunk(i, core)
                mg_copy(d, t, h, j, 1).wait_recv()
                if t == 1:
                    for hop in range(1, 3):
                        if mg_carries(d, t + hop, h):
                            start_all([mg_copy(d, t + hop, h, j, hop)])
                start_all([mgs_copy(i, h, j)])
        if t > 0:
            use_mid(t)
            use_mid(Y - t)
    use_mid(H)

    conv_grad = (mixed[...] * (pre_sig * (1.0 + pre * (1.0 - pre_sig)))).astype(BF16)
    halo_out[...] = conv_grad[:, 0:HW]
    halo = copy_to(
        halo_out, halo_in, halo_send.at[0], halo_recv.at[0], lax.rem(me + S - 1, S), tp
    )
    start_all([halo])
    for m in range(2):
        for b, (src, ref) in enumerate(((send_main, rows), (send_ext, ext))):
            copy_to(
                src.at[m, pl.ds(1, S - 1)],
                ref.at[mine[m], pl.ds(1, S - 1)],
                a2a_send.at[m, b],
                a2a_recv.at[m, b, 0],
                me,
                sib,
            ).wait_send()
    for c in sent[:-1]:
        c.wait_send()
    halo.wait_recv()
    beyond = jnp.where(me == S - 1, 0.0, halo_in[...].astype(F32))
    extended = jnp.concatenate([conv_grad.astype(F32), beyond], axis=1)
    total = taps[:, 0:1] * extended[:, 0:TOK]
    for lag in range(1, KERNEL):
        shifted = pltpu.roll(extended, TOK + HW - lag, 1)
        total = total + taps[:, lag : lag + 1] * shifted[:, 0:TOK]
    conv_in_grad[...] = total

    copy_to(
        proj_out.at[pl.ds(units, (S - 1) * units)],
        proj_in.at[pl.ds(units, (S - 1) * units)],
        proj_send.at[0],
        proj_recv.at[0],
        me,
        sib,
    ).wait()
    for u in range(units):
        z = proj_out[me * units + u].astype(F32)
        for k in range(1, S):
            z = z + proj_in[k * units + u].astype(F32)
        tall = jnp.concatenate([z, pltpu.roll(z, LANES // 2, 1)], axis=0)
        grad_proj[u * (LANES // 2) : (u + 1) * (LANES // 2), :] = tall.T[0 : LANES // 2, :]
    halo.wait_send()


def moe_call(S, T, *args):
    Y = T // 2
    H = Y // 2
    G = max(1, Y // 4)
    TOK, D = args[2].shape
    CC = args[7].shape[0]
    NQ = min(4, S)
    KQ = S // NQ
    R = S * MAIN
    NG = KQ * MAIN + KQ
    HW = min(LANES, TOK)
    vmem = pl.BlockSpec(memory_space=pltpu.VMEM)
    hbm = pl.BlockSpec(memory_space=pltpu.HBM)
    dma = pltpu.SemaphoreType.DMA
    scratch = [
        pltpu.VMEM(args[0].shape, jnp.int32),
        pltpu.VMEM(args[1].shape, F32),
        pltpu.VMEM((2, TOK, LANES), BF16),
        pltpu.VMEM((2, TOK, LANES), BF16),
        pltpu.VMEM((D, LANES), BF16),
        pltpu.VMEM((D, LANES), BF16),
        pltpu.VMEM((LANES, D), BF16),
        pltpu.VMEM(args[7].shape, BF16),
        pltpu.VMEM(args[8].shape, BF16),
        pltpu.VMEM(args[9].shape, BF16),
        dma((12,)),
        pltpu.VMEM((2, S, 2 * MAIN, LANES), BF16),
        pltpu.VMEM((2, S, 2, LANES), BF16),
        pltpu.VMEM((T, S, 2 * MAIN, LANES), BF16),
        pltpu.VMEM((T, S, 2, LANES), BF16),
        pltpu.VMEM((2 * KQ, D), BF16),
        pltpu.VMEM((S, D), F32),
        pltpu.VMEM((S, D), F32),
        pltpu.VMEM((R, TOK), BF16),
        pltpu.VMEM((S, TOK), BF16),
        pltpu.VMEM((R, LANES), BF16),
        pltpu.VMEM((S, LANES), F32),
        pltpu.VMEM((R, 2 * LANES), BF16),
        pltpu.VMEM((S, 2 * LANES), F32),
        pltpu.VMEM((NQ, 2, Y, NG, LANES), BF16),
        pltpu.VMEM((NQ, Y, NG, LANES), BF16),
        pltpu.VMEM((NQ, T, NG, LANES), F32),
        pltpu.VMEM((2, H, NQ, NG, LANES), BF16),
        pltpu.VMEM((2, H, NQ, NG, LANES), BF16),
        pltpu.VMEM((S, MAIN, LANES), BF16),
        pltpu.VMEM((S, 1, LANES), F32),
        pltpu.VMEM((S, MAIN, LANES), BF16),
        pltpu.VMEM((S, 1, LANES), F32),
        pltpu.VMEM((T, TOK, LANES), BF16),
        pltpu.VMEM((CC, TOK), F32),
        pltpu.VMEM((2 * T, CC // 2, LANES), BF16),
        pltpu.VMEM((2 * T, CC // 2, LANES), BF16),
        pltpu.VMEM((CC, HW), BF16),
        pltpu.VMEM((CC, HW), BF16),
        dma((2, 2)),
        dma((2, 2, NQ)),
        dma((2, G, 2, NQ, 2)),
        dma((2, G, 2, NQ, 2)),
        dma((Y, NQ, 2)),
        dma((Y, NQ, 2)),
        dma((NQ,)),
        dma((NQ,)),
        dma((2, H, NQ)),
        dma((2, H, NQ)),
        dma((2,)),
        dma((2,)),
        dma((2, H, 2)),
        dma((2, H, 2)),
        dma((Y, 2)),
        dma((Y, 2)),
        dma((1,)),
        dma((1,)),
        dma((1,)),
        dma((1,)),
    ]
    return pl.pallas_call(
        functools.partial(moe_kernel, S, T, NQ),
        out_shape=(
            jax.ShapeDtypeStruct((D, LANES), BF16),
            jax.ShapeDtypeStruct((D, LANES), BF16),
            jax.ShapeDtypeStruct((LANES, D), BF16),
            jax.ShapeDtypeStruct((D // S, CC), F32),
            jax.ShapeDtypeStruct((CC, TOK), F32),
        ),
        in_specs=[hbm] * len(args),
        out_specs=(vmem,) * 5,
        scratch_shapes=scratch,
        compiler_params=pltpu.CompilerParams(
            collective_id=0, has_side_effects=True, vmem_limit_bytes=36 * 1024 * 1024
        ),
    )(*[pltpu.with_memory_space_constraint(a, pltpu.HBM) for a in args])


def settle_kernel(*refs):
    n = len(refs) // 2
    copies = [
        pltpu.make_async_copy(refs[k], refs[n + k], refs[-1].at[k]) for k in range(n)
    ]
    for c in copies:
        c.start()
    for c in copies:
        c.wait()


def settle(*arrays):
    return pl.pallas_call(
        settle_kernel,
        out_shape=tuple(jax.ShapeDtypeStruct(a.shape, a.dtype) for a in arrays),
        in_specs=[pl.BlockSpec(memory_space=pltpu.VMEM)] * len(arrays),
        out_specs=(pl.BlockSpec(memory_space=pltpu.HBM),) * len(arrays),
        scratch_shapes=[pltpu.SemaphoreType.DMA((len(arrays),))],
        compiler_params=pltpu.CompilerParams(vmem_limit_bytes=8 * 1024 * 1024),
    )(*arrays)


def body(
    S,
    T,
    mid_state,
    conv_pre,
    conv_taps,
    out_proj,
    route_expert,
    route_weight,
    gate_w,
    up_w,
    down_w,
    cotangent,
):
    results = moe_call(
        S,
        T,
        route_expert.T,
        route_weight.T,
        mid_state,
        cotangent,
        gate_w[0],
        up_w[0],
        down_w[0],
        conv_pre.T,
        conv_taps,
        out_proj,
    )
    grad_gate, grad_up, grad_down, grad_proj, conv_in_grad = settle(*results)
    return (grad_gate[None], grad_up[None], grad_down[None], grad_proj, conv_in_grad.T)


def solution(mesh):
    placed = (
        P("sp", None),
        P("sp", "tp"),
        P(None, "tp"),
        P("tp", None),
        P("sp", None),
        P("sp", None),
        P("sp", None, "tp"),
        P("sp", None, "tp"),
        P("sp", "tp", None),
        P("sp", None),
    )
    return jax.shard_map(
        functools.partial(body, mesh.shape["sp"], mesh.shape["tp"]),
        mesh=mesh,
        in_specs=placed,
        out_specs=(
            P("sp", None, "tp"),
            P("sp", None, "tp"),
            P("sp", "tp", None),
            P("sp", "tp"),
            P("sp", "tp"),
        ),
        check_vma=False,
    )
```

```python
import functools

import jax
import jax.numpy as jnp
from jax import lax
from jax.experimental import pallas as pl
from jax.experimental.pallas import tpu as pltpu
from jax.sharding import PartitionSpec as P

KERNEL = 31
LANES = 128
MAIN = 16
MESH = pl.DeviceIdType.MESH
F32 = jnp.float32
BF16 = jnp.bfloat16


def copy_to(src, dst, send, recv, sp, tp):
    return pltpu.make_async_remote_copy(
        src_ref=src,
        dst_ref=dst,
        send_sem=send,
        recv_sem=recv,
        device_id=(sp, tp),
        device_id_type=MESH,
    )


def moe_kernel(
    S,
    T,
    NQ,
    route_e_hbm,
    route_w_hbm,
    mid_hbm,
    cot_hbm,
    gate_hbm,
    up_hbm,
    down_hbm,
    conv_pre_hbm,
    conv_taps_hbm,
    out_proj_hbm,
    grad_gate,
    grad_up,
    grad_down,
    grad_proj,
    conv_in_grad,
    route_e,
    route_w,
    mid,
    cot,
    gate_w,
    up_w,
    down_w,
    conv_pre,
    conv_taps,
    out_proj,
    load_sem,
    send_main,
    send_ext,
    rows,
    ext,
    ext_flat,
    ext_in,
    ext_seed,
    onehot,
    onehot_x,
    hid_main,
    hid_ext,
    pre_main,
    pre_ext,
    sib_out,
    sib_in,
    own_part,
    ring_out,
    ring_in,
    back_main,
    back_ext,
    home_main,
    home_ext,
    gathered,
    mixed,
    proj_out,
    proj_in,
    halo_out,
    halo_in,
    a2a_send,
    a2a_recv,
    ag_send,
    ag_recv,
    sib_send,
    sib_recv,
    rsib_send,
    rsib_recv,
    rs_send,
    rs_recv,
    ret_send,
    ret_recv,
    mg_send,
    mg_recv,
    mgs_send,
    mgs_recv,
    proj_send,
    proj_recv,
    halo_send,
    halo_recv,
):
    Y = T // 2
    H = Y // 2
    G = Y // 4
    KQ = S // NQ
    R = S * MAIN
    RQ = KQ * MAIN
    NG = RQ + KQ
    TOK = mid.shape[1]
    CC = conv_pre.shape[0]
    HW = halo_out.shape[1]
    me = lax.axis_index("sp")
    tp = lax.axis_index("tp")
    y = tp // 2
    core = tp % 2
    sib = tp + 1 - 2 * core
    right = lax.rem(tp + 2, T)
    left = lax.rem(tp + T - 2, T)
    peers = (right, left)
    peers2 = (lax.rem(tp + 4, T), lax.rem(tp + T - 4 + T, T))
    tp2 = lax.rem(tp + H * 2, T)
    mine = (tp, tp2)

    X = 4 if S >= 16 else 1
    Z = S // X
    mz = me // X
    mx = me % X

    def apart(b, sign):
        c = b // X
        zo = jnp.where(c % 2 == 1, (c + 1) // 2, -(c // 2))
        return lax.rem(mz + sign * zo + Z, Z) * X + lax.rem(mx + sign * (b % X) + X, X)

    def chunk(i, parity):
        return 2 * lax.rem(y - i + 2 * Y, Y) + parity

    def lanes(j, width=1):
        return pl.ds(pl.multiple_of(j * LANES, LANES * width), LANES * width)

    barrier = pltpu.get_barrier_semaphore()

    @pl.loop(1, S)
    def _(k):
        pl.semaphore_signal(
            barrier, inc=1, device_id=(apart(k, 1), tp), device_id_type=MESH
        )

    for peer in (left, right, sib) + (peers2 if H > 1 else ()):
        pl.semaphore_signal(barrier, inc=1, device_id=(me, peer), device_id_type=MESH)

    loads = [
        pltpu.make_async_copy(src, dst, load_sem.at[n])
        for n, (src, dst) in enumerate(
            [
                (route_e_hbm, route_e),
                (route_w_hbm, route_w),
                (mid_hbm.at[:, lanes(tp)], mid.at[0]),
                (mid_hbm.at[:, lanes(tp2)], mid.at[1]),
                (cot_hbm.at[:, lanes(tp)], cot.at[0]),
                (cot_hbm.at[:, lanes(tp2)], cot.at[1]),
                (gate_hbm, gate_w),
                (up_hbm, up_w),
                (down_hbm, down_w),
                (conv_pre_hbm, conv_pre),
                (conv_taps_hbm, conv_taps),
                (out_proj_hbm, out_proj),
            ]
        )
    ]
    for c in loads:
        c.start()
    for c in loads[0:6]:
        c.wait()

    experts = route_e[...]
    z_rel = experts // X - mz
    z_rel = jnp.where(z_rel < 0, z_rel + Z, z_rel)
    x_rel = experts % X - mx
    x_rel = jnp.where(x_rel < 0, x_rel + X, x_rel)
    turn = jnp.where(2 * z_rel <= Z, jnp.maximum(2 * z_rel - 1, 0), 2 * (Z - z_rel))
    e_rel = turn * X + x_rel
    e_iota = lax.broadcasted_iota(jnp.int32, (S, TOK), 0)
    oh = [e_iota == e_rel[k : k + 1, :] for k in range(2)]
    oh_sum = (oh[0] | oh[1]).astype(F32).astype(BF16)
    before = (
        lax.broadcasted_iota(jnp.int32, (TOK, TOK), 0)
        < lax.broadcasted_iota(jnp.int32, (TOK, TOK), 1)
    ).astype(F32).astype(BF16)
    counts = jnp.dot(oh_sum, before, preferred_element_type=F32)
    main_rows = lax.broadcasted_iota(jnp.int32, (R, TOK), 0)
    ext_rows = lax.broadcasted_iota(jnp.int32, (S, TOK), 0)
    pair_rows = lax.broadcasted_iota(jnp.int32, (2 * S, TOK), 0)
    g_main, g_ext, g_pair = [], [], []
    for k in range(2):
        rank = jnp.sum(jnp.where(oh[k], counts, 0.0), axis=0, keepdims=True).astype(jnp.int32)
        own = e_rel[k : k + 1, :]
        key = jnp.where(rank < MAIN, own * MAIN + rank, -1)
        key_x = jnp.where(rank == MAIN, own, -1)
        g_main.append(main_rows == key)
        g_ext.append(ext_rows == key_x)
        g_pair.append(pair_rows == 2 * key_x + 1)
    w = [route_w[k : k + 1, :] for k in range(2)]
    gm = (g_main[0] | g_main[1]).astype(F32).astype(BF16)
    onehot[...] = gm
    onehot_x[...] = (g_ext[0] | g_ext[1]).astype(F32).astype(BF16)
    mid_c = jnp.concatenate([mid[0], mid[1]], axis=1)
    cot_c = jnp.concatenate([cot[0], cot[1]], axis=1)
    w_main = jnp.sum(
        jnp.where(g_main[0], w[0], 0.0) + jnp.where(g_main[1], w[1], 0.0), axis=1, keepdims=True
    )
    in_rows = jnp.dot(gm, mid_c, preferred_element_type=F32).astype(BF16)
    seed_rows = (w_main * jnp.dot(gm, cot_c, preferred_element_type=F32)).astype(BF16)
    w_pair = jnp.sum(
        jnp.where(g_pair[0], w[0], 0.0) + jnp.where(g_pair[1], w[1], 0.0), axis=1, keepdims=True
    )
    g_odd = (g_pair[0] | g_pair[1]).astype(F32).astype(BF16)
    pair_even = lax.broadcasted_iota(jnp.int32, (2 * S, S), 0) == 2 * lax.broadcasted_iota(
        jnp.int32, (2 * S, S), 1
    )
    g_even = jnp.dot(
        pair_even.astype(F32).astype(BF16), onehot_x[...], preferred_element_type=F32
    ).astype(BF16)
    pair_val = (
        jnp.dot(g_even, mid_c, preferred_element_type=F32)
        + w_pair * jnp.dot(g_odd, cot_c, preferred_element_type=F32)
    ).astype(BF16)
    for m in range(2):
        part = slice(m * LANES, (m + 1) * LANES)
        send_main[m, :, 0:MAIN, :] = in_rows[:, part].reshape(S, MAIN, LANES)
        send_main[m, :, MAIN : 2 * MAIN, :] = seed_rows[:, part].reshape(S, MAIN, LANES)
        for s in range(S):
            send_ext[m, s] = pair_val[2 * s : 2 * s + 2, part]

    pl.semaphore_wait(barrier, S + 2 + (2 if H > 1 else 0))

    @pl.loop(1, S)
    def _(k):
        dst = apart(k, 1)
        q = k // KQ
        for m in range(2):
            for b, (src, ref) in enumerate(((send_main, rows), (send_ext, ext))):
                copy_to(
                    src.at[m, k],
                    ref.at[mine[m], k],
                    a2a_send.at[m, b],
                    a2a_recv.at[m, b, q],
                    dst,
                    tp,
                ).start()

    for m in range(2):
        rows[mine[m], 0] = send_main[m, 0]
        ext[mine[m], 0] = send_ext[m, 0]

    both = (rows, ext)
    sent = []

    def start_all(copies):
        for c in copies:
            c.start()
        sent.extend(copies)

    def sub(ref, j, q):
        return ref.at[j, pl.ds(q * KQ, KQ)]

    def ag_copies(d, t, m, q, j):
        return [
            copy_to(
                sub(ref, j, q),
                sub(ref, j, q),
                ag_send.at[d, t, m, q, b],
                ag_recv.at[d, t, m, q, b],
                me,
                peers[d],
            )
            for b, ref in enumerate(both)
        ]

    def sib_copies(i, q, j):
        return [
            copy_to(
                sub(ref, j, q), sub(ref, j, q), sib_send.at[i, q, b], sib_recv.at[i, q, b], me, sib
            )
            for b, ref in enumerate(both)
        ]

    def hops(m):
        return G - m

    def near(d, t, m):
        return ((t + 1) if d == 0 else Y - (t + 1)) + m * H

    def slot_of(i):
        return i % Y

    def step_a(q):
        lo = 1 if q == 0 else q * KQ
        n = (q + 1) * KQ - lo
        if n > 0:
            for m in range(2):
                for b, (src, ref) in enumerate(((send_main, rows), (send_ext, ext))):
                    copy_to(
                        src.at[m, pl.ds(lo, n)],
                        ref.at[mine[m], pl.ds(lo, n)],
                        a2a_send.at[m, b],
                        a2a_recv.at[m, b, q],
                        me,
                        sib,
                    ).wait_recv()
        for m in range(2):
            for d in range(2):
                if hops(m) > 0:
                    start_all(ag_copies(d, 0, m, q, mine[m]))
        for m in range(2):
            start_all(sib_copies(m * H, q, mine[m]))

    def arrive(d, t, m, q):
        i = slot_of(near(d, t, m))
        j = chunk(i, core)
        for c in ag_copies(d, t, m, q, j):
            c.wait_recv()
        if t + 1 < hops(m):
            start_all(ag_copies(d, t + 1, m, q, j))
        start_all(sib_copies(i, q, j))

    def step_f(q):
        for m in range(2):
            for d in range(2):
                if hops(m) > 0:
                    arrive(d, 0, m, q)

    def step_e(q):
        for t in range(1, G):
            for m in range(2):
                for d in range(2):
                    if t < hops(m):
                        arrive(d, t, m, q)

    sel_row = lax.broadcasted_iota(jnp.int32, (KQ, 2 * KQ), 0)
    sel_col = lax.broadcasted_iota(jnp.int32, (KQ, 2 * KQ), 1)
    sels = [(sel_col == 2 * sel_row + b).astype(F32).astype(BF16) for b in range(2)]

    def rsib_copy(q):
        return copy_to(
            sib_out.at[q, 1 - core], sib_in.at[q], rsib_send.at[q], rsib_recv.at[q], me, sib
        )

    def step_c(q):
        for i in range(Y):
            for c in sib_copies(i, q, chunk(i, 1 - core)):
                c.wait_recv()
        if q == 0:
            for c in loads[6:9]:
                c.wait()
        for j in range(T):
            for s in range(KQ):
                ext_flat[2 * s : 2 * s + 2, j * LANES : (j + 1) * LANES] = ext[j, q * KQ + s]
        flat = ext_flat[...]
        ext_q = slice(q * KQ, (q + 1) * KQ)
        x_ext = jnp.dot(sels[0], flat, preferred_element_type=F32)
        s_ext = jnp.dot(sels[1], flat, preferred_element_type=F32)
        ext_in[ext_q, :] = x_ext
        ext_seed[ext_q, :] = s_ext
        x = jnp.concatenate(
            [rows[j, q * KQ : (q + 1) * KQ, 0:MAIN, :].reshape(RQ, LANES) for j in range(T)],
            axis=1,
        )
        x = jnp.concatenate([x, x_ext.astype(BF16)], axis=0)
        g = jnp.concatenate(
            [
                rows[j, q * KQ : (q + 1) * KQ, MAIN : 2 * MAIN, :].reshape(RQ, LANES)
                for j in range(T)
            ],
            axis=1,
        )
        g = jnp.concatenate([g, s_ext.astype(BF16)], axis=0)
        w_gu = jnp.concatenate([gate_w[...], up_w[...]], axis=1)
        gate_up = jnp.dot(x, w_gu, preferred_element_type=F32)
        gate_pre = gate_up[:, 0:LANES]
        up_pre = gate_up[:, LANES : 2 * LANES]
        h_grad = lax.dot_general(
            g, down_w[...], (((1,), (1,)), ((), ())), preferred_element_type=F32
        )
        sig = jax.nn.sigmoid(gate_pre)
        act = gate_pre * sig
        hid = (act * up_pre).astype(BF16)
        gate_g = (h_grad * up_pre * (sig * (1.0 + gate_pre * (1.0 - sig)))).astype(BF16)
        pre = jnp.concatenate([gate_g, (h_grad * act).astype(BF16)], axis=1)
        hid_main[q * RQ : (q + 1) * RQ, :] = hid[0:RQ]
        hid_ext[ext_q, :] = hid[RQ:NG].astype(F32)
        pre_main[q * RQ : (q + 1) * RQ, :] = pre[0:RQ]
        pre_ext[ext_q, :] = pre[RQ:NG].astype(F32)

        parts = lax.dot_general(pre, w_gu, (((1,), (1,)), ((), ())), preferred_element_type=F32)
        for j in range(T):
            value = parts[:, j * LANES : (j + 1) * LANES]
            own_part[q, j] = value
            sib_out[q, j % 2, j // 2] = value.astype(BF16)
        start_all([rsib_copy(q)])

    def rs_copy(d, t, q):
        return copy_to(
            ring_out.at[d, t, q],
            ring_in.at[d, t, q],
            rs_send.at[d, t, q],
            rs_recv.at[d, t, q],
            me,
            peers[d],
        )

    def rs_has(d, t, q):
        if t < 0:
            return False
        return t > 0 or q % 2 == d

    def step_b(q, t):
        if t == 0:
            rsib_copy(q).wait_recv()
        if t == H:
            value = own_part[q, tp] + sib_in[q, y].astype(F32)
            for d in range(2):
                if rs_has(d, H - 1, q):
                    rs_copy(d, H - 1, q).wait_recv()
                    value = value + ring_in[d, H - 1, q].astype(F32)
            value = value.astype(BF16)
            back_main[q * KQ : (q + 1) * KQ] = value[0:RQ].reshape(KQ, MAIN, LANES)
            last = value[RQ:NG].astype(F32)
            for s in range(KQ):
                back_ext[q * KQ + s] = last[s : s + 1, :]
            if q == 0:
                home_main[0] = back_main[0]
                home_ext[0] = back_ext[0]

            @pl.loop(max(1, q * KQ), (q + 1) * KQ)
            def _(k):
                dst = apart(k, -1)
                for b, (src, ref) in enumerate(((back_main, home_main), (back_ext, home_ext))):
                    copy_to(
                        src.at[k], ref.at[k], ret_send.at[b], ret_recv.at[b], dst, tp
                    ).start()

            return
        dist = H - t
        for d in range(2):
            if not rs_has(d, t, q):
                continue
            o = dist if d == 0 else Y - dist
            to = lax.rem(y + o, Y)
            value = own_part[q, 2 * to + core] + sib_in[q, to].astype(F32)
            if rs_has(d, t - 1, q):
                rs_copy(d, t - 1, q).wait_recv()
                value = value + ring_in[d, t - 1, q].astype(F32)
            ring_out[d, t, q] = value.astype(BF16)
            start_all([rs_copy(d, t, q)])

    def weight_grads(j):
        x = jnp.concatenate(
            [rows[j, :, 0:MAIN, :].reshape(R, LANES), ext_in[:, lanes(j)].astype(BF16)], axis=0
        )
        g = jnp.concatenate(
            [
                rows[j, :, MAIN : 2 * MAIN, :].reshape(R, LANES),
                ext_seed[:, lanes(j)].astype(BF16),
            ],
            axis=0,
        )
        pre = jnp.concatenate([pre_main[...], pre_ext[...].astype(BF16)], axis=0)
        hid = jnp.concatenate([hid_main[...], hid_ext[...].astype(BF16)], axis=0)
        both_g = lax.dot_general(
            x, pre, (((0,), (0,)), ((), ())), preferred_element_type=F32
        ).astype(BF16)
        grad_gate[lanes(j), :] = both_g[:, 0:LANES]
        grad_up[lanes(j), :] = both_g[:, LANES : 2 * LANES]
        grad_down[:, lanes(j)] = lax.dot_general(
            hid, g, (((0,), (0,)), ((), ())), preferred_element_type=F32
        ).astype(BF16)

    reached = [-1] * NQ
    ready = [0]

    def round_b():
        for q in range(ready[0]):
            if reached[q] < H:
                reached[q] += 1
                step_b(q, reached[q])

    step_a(0)
    for q in range(1, NQ + 3):
        if q < NQ:
            step_a(q)
        if 0 <= q - 1 < NQ:
            step_f(q - 1)
        if 0 <= q - 2 < NQ:
            step_e(q - 2)
        if 0 <= q - 3 < NQ:
            step_c(q - 3)
            ready[0] += 1
    done = 0
    for s in range(H + 1):
        round_b()
        stop = T * (s + 1) // (H + 1)

        @pl.loop(done, stop)
        def _(j):
            weight_grads(j)

        done = stop

    for c in loads[9:12]:
        c.wait()
    pre = conv_pre[...].astype(F32)
    pre_sig = jax.nn.sigmoid(pre)
    activated = (pre * pre_sig).astype(BF16)
    eye = (
        lax.broadcasted_iota(jnp.int32, (KERNEL, KERNEL), 0)
        == lax.broadcasted_iota(jnp.int32, (KERNEL, KERNEL), 1)
    ).astype(F32).astype(BF16)
    taps = lax.dot_general(
        conv_taps[...], eye, (((0,), (0,)), ((), ())), preferred_element_type=F32
    )
    for b, (src, ref) in enumerate(((back_main, home_main), (back_ext, home_ext))):
        copy_to(
            src.at[pl.ds(1, S - 1)],
            ref.at[pl.ds(1, S - 1)],
            ret_send.at[b],
            ret_recv.at[b],
            me,
            sib,
        ).wait()
    home_x = jnp.concatenate([home_ext[s] for s in range(S)], axis=0).astype(BF16)
    moe = lax.dot_general(
        onehot[...],
        home_main[...].reshape(R, LANES),
        (((0,), (0,)), ((), ())),
        preferred_element_type=F32,
    ) + lax.dot_general(
        onehot_x[...], home_x, (((0,), (0,)), ((), ())), preferred_element_type=F32
    )
    gathered[tp] = (cot[0].astype(F32) + moe).astype(BF16)

    TH = TOK // 2

    def mg_copy(d, t, h, j, hop):
        part = gathered.at[j, pl.ds(h * TH, TH)]
        peer = peers[d] if hop == 1 else peers2[d]
        return copy_to(part, part, mg_send.at[d, t, h], mg_recv.at[d, t, h], me, peer)

    def mgs_copy(i, h, j):
        part = gathered.at[j, pl.ds(h * TH, TH)]
        return copy_to(part, part, mgs_send.at[i, h], mgs_recv.at[i, h], me, sib)

    def mg_carries(d, t, h):
        if t + 1 < H:
            return True
        if t + 1 > H:
            return False
        return h == d

    mixed[...] = jnp.zeros_like(mixed)
    units = proj_out.shape[0] // S
    low = lax.broadcasted_iota(jnp.int32, (CC // 2, LANES), 1) < LANES // 2

    def use_mid(i):
        for h in range(2):
            mgs_copy(i, h, chunk(i, 1 - core)).wait_recv()
        j0 = chunk(i, 0)
        g = jnp.concatenate([gathered[j0], gathered[j0 + 1]], axis=1)
        mixed[...] += lax.dot_general(
            out_proj[:, lanes(j0, 2)], g, (((1,), (1,)), ((), ())), preferred_element_type=F32
        )
        part = jnp.dot(activated, g, preferred_element_type=F32)
        for p in range(2):
            top = part[0 : CC // 2, p * LANES : (p + 1) * LANES]
            low_c = part[CC // 2 : CC, p * LANES : (p + 1) * LANES]
            proj_out[2 * (j0 + p)] = jnp.where(
                low, top, pltpu.roll(low_c, LANES // 2, 1)
            ).astype(BF16)
            proj_out[2 * (j0 + p) + 1] = jnp.where(
                low, pltpu.roll(top, LANES // 2, 1), low_c
            ).astype(BF16)
        for p in range(4):
            u = 2 * j0 + p
            dst = u // units
            k = lax.rem(dst - me + S, S)

            @pl.when(k > 0)
            def _():
                copy_to(
                    proj_out.at[u],
                    proj_in.at[k * units + lax.rem(u, units)],
                    proj_send.at[0],
                    proj_recv.at[0],
                    dst,
                    tp,
                ).start()

    for hop in (2, 1):
        for h in range(2):
            for d in range(2):
                if mg_carries(d, hop - 1, h):
                    start_all([mg_copy(d, hop - 1, h, tp, hop)])
            if hop == 1:
                start_all([mgs_copy(0, h, tp)])
    use_mid(0)
    for t in range(H):
        for h in range(2):
            for d in range(2):
                if not mg_carries(d, t, h):
                    continue
                i = t + 1 if d == 0 else Y - (t + 1)
                j = chunk(i, core)
                mg_copy(d, t, h, j, 1).wait_recv()
                if t == 1:
                    for hop in (2, 1):
                        if mg_carries(d, t + hop, h):
                            start_all([mg_copy(d, t + hop, h, j, hop)])
                start_all([mgs_copy(i, h, j)])
        if t > 0:
            use_mid(t)
            use_mid(Y - t)
    use_mid(H)

    conv_grad = (mixed[...] * (pre_sig * (1.0 + pre * (1.0 - pre_sig)))).astype(BF16)
    halo_out[...] = conv_grad[:, 0:HW]
    halo = copy_to(
        halo_out, halo_in, halo_send.at[0], halo_recv.at[0], lax.rem(me + S - 1, S), tp
    )
    start_all([halo])
    for m in range(2):
        for b, (src, ref) in enumerate(((send_main, rows), (send_ext, ext))):
            copy_to(
                src.at[m, pl.ds(1, S - 1)],
                ref.at[mine[m], pl.ds(1, S - 1)],
                a2a_send.at[m, b],
                a2a_recv.at[m, b, 0],
                me,
                sib,
            ).wait_send()
    for c in sent[:-1]:
        c.wait_send()
    halo.wait_recv()
    beyond = jnp.where(me == S - 1, 0.0, halo_in[...].astype(F32))
    extended = jnp.concatenate([conv_grad.astype(F32), beyond], axis=1)
    total = taps[:, 0:1] * extended[:, 0:TOK]
    for lag in range(1, KERNEL):
        shifted = pltpu.roll(extended, TOK + HW - lag, 1)
        total = total + taps[:, lag : lag + 1] * shifted[:, 0:TOK]
    conv_in_grad[...] = total

    copy_to(
        proj_out.at[pl.ds(units, (S - 1) * units)],
        proj_in.at[pl.ds(units, (S - 1) * units)],
        proj_send.at[0],
        proj_recv.at[0],
        me,
        sib,
    ).wait()
    for u in range(units):
        z = proj_out[me * units + u].astype(F32)
        for k in range(1, S):
            z = z + proj_in[k * units + u].astype(F32)
        tall = jnp.concatenate([z, pltpu.roll(z, LANES // 2, 1)], axis=0)
        grad_proj[u * (LANES // 2) : (u + 1) * (LANES // 2), :] = tall.T[0 : LANES // 2, :]
    halo.wait_send()


def moe_call(S, T, *args):
    Y = T // 2
    H = Y // 2
    G = max(1, Y // 4)
    TOK, D = args[2].shape
    CC = args[7].shape[0]
    NQ = min(4, S)
    KQ = S // NQ
    R = S * MAIN
    NG = KQ * MAIN + KQ
    HW = min(LANES, TOK)
    vmem = pl.BlockSpec(memory_space=pltpu.VMEM)
    hbm = pl.BlockSpec(memory_space=pltpu.HBM)
    dma = pltpu.SemaphoreType.DMA
    scratch = [
        pltpu.VMEM(args[0].shape, jnp.int32),
        pltpu.VMEM(args[1].shape, F32),
        pltpu.VMEM((2, TOK, LANES), BF16),
        pltpu.VMEM((2, TOK, LANES), BF16),
        pltpu.VMEM((D, LANES), BF16),
        pltpu.VMEM((D, LANES), BF16),
        pltpu.VMEM((LANES, D), BF16),
        pltpu.VMEM(args[7].shape, BF16),
        pltpu.VMEM(args[8].shape, BF16),
        pltpu.VMEM(args[9].shape, BF16),
        dma((12,)),
        pltpu.VMEM((2, S, 2 * MAIN, LANES), BF16),
        pltpu.VMEM((2, S, 2, LANES), BF16),
        pltpu.VMEM((T, S, 2 * MAIN, LANES), BF16),
        pltpu.VMEM((T, S, 2, LANES), BF16),
        pltpu.VMEM((2 * KQ, D), BF16),
        pltpu.VMEM((S, D), F32),
        pltpu.VMEM((S, D), F32),
        pltpu.VMEM((R, TOK), BF16),
        pltpu.VMEM((S, TOK), BF16),
        pltpu.VMEM((R, LANES), BF16),
        pltpu.VMEM((S, LANES), F32),
        pltpu.VMEM((R, 2 * LANES), BF16),
        pltpu.VMEM((S, 2 * LANES), F32),
        pltpu.VMEM((NQ, 2, Y, NG, LANES), BF16),
        pltpu.VMEM((NQ, Y, NG, LANES), BF16),
        pltpu.VMEM((NQ, T, NG, LANES), F32),
        pltpu.VMEM((2, H, NQ, NG, LANES), BF16),
        pltpu.VMEM((2, H, NQ, NG, LANES), BF16),
        pltpu.VMEM((S, MAIN, LANES), BF16),
        pltpu.VMEM((S, 1, LANES), F32),
        pltpu.VMEM((S, MAIN, LANES), BF16),
        pltpu.VMEM((S, 1, LANES), F32),
        pltpu.VMEM((T, TOK, LANES), BF16),
        pltpu.VMEM((CC, TOK), F32),
        pltpu.VMEM((2 * T, CC // 2, LANES), BF16),
        pltpu.VMEM((2 * T, CC // 2, LANES), BF16),
        pltpu.VMEM((CC, HW), BF16),
        pltpu.VMEM((CC, HW), BF16),
        dma((2, 2)),
        dma((2, 2, NQ)),
        dma((2, G, 2, NQ, 2)),
        dma((2, G, 2, NQ, 2)),
        dma((Y, NQ, 2)),
        dma((Y, NQ, 2)),
        dma((NQ,)),
        dma((NQ,)),
        dma((2, H, NQ)),
        dma((2, H, NQ)),
        dma((2,)),
        dma((2,)),
        dma((2, H, 2)),
        dma((2, H, 2)),
        dma((Y, 2)),
        dma((Y, 2)),
        dma((1,)),
        dma((1,)),
        dma((1,)),
        dma((1,)),
    ]
    return pl.pallas_call(
        functools.partial(moe_kernel, S, T, NQ),
        out_shape=(
            jax.ShapeDtypeStruct((D, LANES), BF16),
            jax.ShapeDtypeStruct((D, LANES), BF16),
            jax.ShapeDtypeStruct((LANES, D), BF16),
            jax.ShapeDtypeStruct((D // S, CC), F32),
            jax.ShapeDtypeStruct((CC, TOK), F32),
        ),
        in_specs=[hbm] * len(args),
        out_specs=(vmem,) * 5,
        scratch_shapes=scratch,
        compiler_params=pltpu.CompilerParams(
            collective_id=0, has_side_effects=True, vmem_limit_bytes=36 * 1024 * 1024
        ),
    )(*[pltpu.with_memory_space_constraint(a, pltpu.HBM) for a in args])


def settle_kernel(*refs):
    n = len(refs) // 2
    copies = [
        pltpu.make_async_copy(refs[k], refs[n + k], refs[-1].at[k]) for k in range(n)
    ]
    for c in copies:
        c.start()
    for c in copies:
        c.wait()


def settle(*arrays):
    return pl.pallas_call(
        settle_kernel,
        out_shape=tuple(jax.ShapeDtypeStruct(a.shape, a.dtype) for a in arrays),
        in_specs=[pl.BlockSpec(memory_space=pltpu.VMEM)] * len(arrays),
        out_specs=(pl.BlockSpec(memory_space=pltpu.HBM),) * len(arrays),
        scratch_shapes=[pltpu.SemaphoreType.DMA((len(arrays),))],
        compiler_params=pltpu.CompilerParams(vmem_limit_bytes=8 * 1024 * 1024),
    )(*arrays)


def body(
    S,
    T,
    mid_state,
    conv_pre,
    conv_taps,
    out_proj,
    route_expert,
    route_weight,
    gate_w,
    up_w,
    down_w,
    cotangent,
):
    results = moe_call(
        S,
        T,
        route_expert.T,
        route_weight.T,
        mid_state,
        cotangent,
        gate_w[0],
        up_w[0],
        down_w[0],
        conv_pre.T,
        conv_taps,
        out_proj,
    )
    grad_gate, grad_up, grad_down, grad_proj, conv_in_grad = settle(*results)
    return (grad_gate[None], grad_up[None], grad_down[None], grad_proj, conv_in_grad.T)


def solution(mesh):
    placed = (
        P("sp", None),
        P("sp", "tp"),
        P(None, "tp"),
        P("tp", None),
        P("sp", None),
        P("sp", None),
        P("sp", None, "tp"),
        P("sp", None, "tp"),
        P("sp", "tp", None),
        P("sp", None),
    )
    return jax.shard_map(
        functools.partial(body, mesh.shape["sp"], mesh.shape["tp"]),
        mesh=mesh,
        in_specs=placed,
        out_specs=(
            P("sp", None, "tp"),
            P("sp", None, "tp"),
            P("sp", "tp", None),
            P("sp", "tp"),
            P("sp", "tp"),
        ),
        check_vma=False,
    )
```
